32 devices in a mesh: sp: 8 (over z, y), tp: 4 (over x, core).
Axes of the slice: x: 2, y: 2, z: 4, core: 2. Of those that a mesh axis runs over, the one named last changes fastest.
Arguments:
- queries: bfloat16 [6144, 1536], P('sp', 'tp'), may hold values from -130 to 130, as said below
- keys: bfloat16 [6144, 512], P('sp', 'tp'), may hold values from -6 to 6
- values: bfloat16 [6144, 512], P('sp', 'tp'), may hold values from -6 to 6
- residual: bfloat16 [6144, 2048], P(('sp', 'tp')), may hold values from -6 to 6
- sinks: float32 [12], P('tp'), may hold values from 2 to 6
- out_weight: bfloat16 [1536, 2048], P('tp'), may hold values from -0.15625 to 0.15625
- up_weight: bfloat16 [2048, 8192], P('sp', 'tp'), may hold values from -0.125 to 0.125
- down_weight: bfloat16 [8192, 2048], P('tp', 'sp'), may hold values from -0.0625 to 0.0625
- gains: float32 [2, 2048], replicated, may hold values from 0.1 to 1.9
- biases: float32 [2, 2048], replicated, may hold values from -3 to 3
Outputs:
- layer_out: bfloat16 [6144, 2048], P(('sp', 'tp'))
The draws below stay inside these ranges and needn't reach their ends.
Inputs may be any that keep to these rules, and one draw needn't show every extreme that they name: `queries`: entries of order one, with some rows far larger in some draws.
All inputs are finite; a program needn't handle non-finite values.
Results may differ from the reference program's by a relative error of at most 0.0095.
Values may be sent and summed in bfloat16 or wider, within the bound.
A program may use at most 128 MiB of HBM per device.

```python
import jax
import jax.numpy as jnp
from jax import lax

D = 2048
HEADS = 12
KV_HEADS = 4
HEAD = 128
FF = 8192
WINDOW = 128
TOKENS = 6144
Q_W = 1536
KV_W = 512
N_TP = 4


def base_keys(key):
    drawn = jax.random.normal(jax.random.fold_in(key, 11), (TOKENS, KV_HEADS * HEAD), jnp.float32)
    return jnp.clip(drawn, -6.0, 6.0)


def draw_keys(key, part):
    return base_keys(key).astype(jnp.bfloat16)


def draw_queries(key, part):
    drawn = jnp.clip(jax.random.normal(jax.random.fold_in(key, 12), (TOKENS, HEADS * HEAD), jnp.float32), -6.0, 6.0)
    return drawn.astype(jnp.bfloat16)


def shard_levels(own_key, extent, pieces, low, high):
    level = 1.0
    for axis_at, blocks in pieces:
        steps = jax.random.uniform(jax.random.fold_in(jax.random.fold_in(own_key, 6), axis_at), (blocks,), jnp.float32, low / len(pieces), high / len(pieces))
        level = level * jnp.repeat(jnp.exp(steps), extent[axis_at] // blocks).reshape((-1,) + (1,) * (len(extent) - 1 - axis_at))
    return level


def gaussian(stream_key, shape, scale, limit, split=(), kind=jnp.bfloat16):
    entries = jax.random.normal(stream_key, shape, jnp.float32) * scale
    if len(split) > 0:
        entries = shard_levels(stream_key, shape, split, -0.22, 0.18) * entries
    return jnp.clip(entries, min=-limit, max=limit).astype(kind)


def setup_inputs(seed: int = 0) -> dict:
    streams_of = jax.random.split(jax.random.key(seed), 11)
    return {
        "queries": draw_queries(jax.random.fold_in(streams_of[10], 71), 0),
        "keys": draw_keys(jax.random.fold_in(streams_of[10], 71), 0),
        "values": gaussian(streams_of[2], (TOKENS, KV_W), 1.0, 6.0, ((0, 8), (1, 4))),
        "residual": gaussian(streams_of[3], (TOKENS, D), 1.0, 6.0, ((0, 32),)),
        "sinks": jnp.clip(2.0 + 4.0 * jax.random.uniform(streams_of[4], (HEADS,), jnp.float32) ** shard_levels(streams_of[4], (HEADS,), ((0, 4),), -0.2, 0.2), 2.0, 6.0),
        "out_weight": gaussian(streams_of[5], (Q_W, D), Q_W ** -0.5, 0.15625, ((0, 4),)),
        "up_weight": gaussian(streams_of[6], (D, FF), D ** -0.5, 0.125, ((0, 8), (1, 4))),
        "down_weight": gaussian(streams_of[7], (FF, D), FF ** -0.5, 0.0625, ((0, 4), (1, 8))),
        "gains": jnp.clip(1.0 + 0.18 * jax.random.normal(streams_of[8], (2, D), jnp.float32), 0.1, 1.9),
        "biases": gaussian(streams_of[9], (2, D), 0.5, 3.0, (), jnp.float32),
    }


deep_alpha = 1.6817928
norm_eps = 1e-05
neg_big = -1e+30

def layer_norm(stream, gain, bias):
    mean = lax.optimization_barrier(jnp.mean(stream, axis=-1, keepdims=True))
    spread = lax.optimization_barrier(jnp.mean(jnp.square(stream - mean), axis=-1, keepdims=True))
    return ((stream - mean) * lax.rsqrt(spread + norm_eps) * gain + bias).astype(jnp.bfloat16)

def window_attention(queries, keys, values, sinks):
    total = keys.shape[0]
    blocks = total // WINDOW
    group = HEADS // KV_HEADS
    q_blocks = queries.reshape(blocks, WINDOW, KV_HEADS, group, HEAD).astype(jnp.float32)
    padding = jnp.zeros((WINDOW, KV_HEADS, HEAD), jnp.bfloat16)
    key_ext = jnp.concatenate([padding, keys.reshape(total, KV_HEADS, HEAD)], axis=0)
    val_ext = jnp.concatenate([padding, values.reshape(total, KV_HEADS, HEAD)], axis=0)
    key_win = jnp.concatenate([key_ext[:total].reshape(blocks, WINDOW, KV_HEADS, HEAD), key_ext[WINDOW:].reshape(blocks, WINDOW, KV_HEADS, HEAD)], axis=1)
    val_win = jnp.concatenate([val_ext[:total].reshape(blocks, WINDOW, KV_HEADS, HEAD), val_ext[WINDOW:].reshape(blocks, WINDOW, KV_HEADS, HEAD)], axis=1)
    logits = jnp.einsum('nqkgd,nskd->nkgqs', q_blocks, key_win.astype(jnp.float32)) * HEAD ** (-0.5)
    q_index = jnp.arange(WINDOW, dtype=jnp.int32)[:, None]
    k_index = jnp.arange(2 * WINDOW, dtype=jnp.int32)[None, :]
    dist = q_index + WINDOW - k_index
    block_id = jnp.arange(blocks, dtype=jnp.int32)[:, None, None]
    key_pos = block_id * WINDOW - WINDOW + k_index
    valid = (dist >= 0) & (dist < WINDOW) & (key_pos >= 0)
    heads = jnp.arange(HEADS, dtype=jnp.float32)
    slopes = jnp.exp2(-8.0 * (heads + 1.0) / HEADS).reshape(KV_HEADS, group)[:, :, None, None]
    logits = logits - slopes * dist.astype(jnp.float32)
    logits = jnp.where(valid[:, None, None], logits, neg_big)
    sink = sinks.reshape(KV_HEADS, group)[:, :, None, None]
    top = jnp.maximum(lax.optimization_barrier(jnp.max(logits, axis=-1, keepdims=True)), sink)
    probs = jnp.exp(logits - top)
    denom = lax.optimization_barrier(jnp.sum(probs, axis=-1, keepdims=True)) + jnp.exp(sink - top)
    weight = (probs / denom).astype(jnp.bfloat16)
    attended = jnp.einsum('nkgqs,nskd->nqkgd', weight.astype(jnp.float32), val_win.astype(jnp.float32))
    return attended.astype(jnp.bfloat16).reshape(total, Q_W)

def reference(queries, keys, values, residual, sinks, out_weight, up_weight, down_weight, gains, biases):
    attended = window_attention(queries, keys, values, sinks)
    width = Q_W // N_TP
    mix = jnp.zeros((TOKENS, D), jnp.float32)
    for group_id in range(N_TP):
        term = jnp.dot(attended[:, group_id * width:(group_id + 1) * width], out_weight[group_id * width:(group_id + 1) * width], preferred_element_type=jnp.float32).astype(jnp.bfloat16)
        mix = mix + term.astype(jnp.float32)
    normed = layer_norm(deep_alpha * residual.astype(jnp.float32) + mix, gains[0], biases[0])
    hidden = FF // N_TP
    ffn = jnp.zeros((TOKENS, D), jnp.float32)
    for group_id in range(N_TP):
        upward = jnp.dot(normed, up_weight[:, group_id * hidden:(group_id + 1) * hidden], preferred_element_type=jnp.float32)
        act = jnp.square(jax.nn.relu(upward)).astype(jnp.bfloat16)
        term = jnp.dot(act, down_weight[group_id * hidden:(group_id + 1) * hidden], preferred_element_type=jnp.float32).astype(jnp.bfloat16)
        ffn = ffn + term.astype(jnp.float32)
    return layer_norm(deep_alpha * normed.astype(jnp.float32) + ffn, gains[1], biases[1])
```

```python
import functools

import jax
import jax.numpy as jnp
from jax import lax
from jax.experimental import pallas as pl
from jax.experimental.pallas import tpu as pltpu
from jax.sharding import PartitionSpec as P

HEADS = 12
HEAD = 128
WINDOW = 128


deep_alpha = 1.6817928
norm_eps = 1e-05
neg_big = -1e30


def from_behind(block, axis, distance):
    devices = range(lax.axis_size(axis))
    route = [(i - distance, i) for i in devices if i - distance in devices]
    return lax.ppermute(block, axis, route)


def layer_norm(stream, gain, bias):
    mean = jnp.mean(stream, axis=-1, keepdims=True)
    spread = jnp.mean(jnp.square(stream - mean), axis=-1, keepdims=True)
    return ((stream - mean) * lax.rsqrt(spread + norm_eps) * gain + bias).astype(jnp.bfloat16)


def attend(queries, keys, values, before, sinks, offset, rank_tp):
    tokens = keys.shape[0]
    kv_local = keys.shape[1] // HEAD
    heads_local = sinks.shape[0]
    group = heads_local // kv_local
    blocks = tokens // WINDOW
    q_blocks = queries.reshape(blocks, WINDOW, kv_local, group, HEAD)
    key_ext = jnp.concatenate([before[0], keys], axis=0).reshape(tokens + WINDOW, kv_local, HEAD)
    val_ext = jnp.concatenate([before[1], values], axis=0).reshape(tokens + WINDOW, kv_local, HEAD)
    key_win = jnp.concatenate(
        [
            key_ext[:tokens].reshape(blocks, WINDOW, kv_local, HEAD),
            key_ext[WINDOW:].reshape(blocks, WINDOW, kv_local, HEAD),
        ],
        axis=1,
    )
    val_win = jnp.concatenate(
        [
            val_ext[:tokens].reshape(blocks, WINDOW, kv_local, HEAD),
            val_ext[WINDOW:].reshape(blocks, WINDOW, kv_local, HEAD),
        ],
        axis=1,
    )
    logits = jnp.einsum(
        "nqkgd,nskd->nkgqs", q_blocks, key_win, preferred_element_type=jnp.float32
    ) * HEAD ** (-0.5)
    q_index = jnp.arange(WINDOW, dtype=jnp.int32)[:, None]
    k_index = jnp.arange(2 * WINDOW, dtype=jnp.int32)[None, :]
    dist = q_index + WINDOW - k_index
    block_id = jnp.arange(blocks, dtype=jnp.int32)[:, None, None]
    key_pos = offset + block_id * WINDOW - WINDOW + k_index
    valid = (dist >= 0) & (dist < WINDOW) & (key_pos >= 0)
    heads = (jnp.arange(heads_local, dtype=jnp.int32) + rank_tp * heads_local).astype(jnp.float32)
    slopes = jnp.exp2(-8.0 * (heads + 1.0) / HEADS).reshape(kv_local, group)[:, :, None, None]
    logits = logits - slopes * dist.astype(jnp.float32)
    logits = jnp.where(valid[:, None, None], logits, neg_big)
    sink = sinks.reshape(kv_local, group)[:, :, None, None]
    top = jnp.maximum(jnp.max(logits, axis=-1, keepdims=True), sink)
    probs = jnp.exp(logits - top)
    denom = jnp.sum(probs, axis=-1, keepdims=True) + jnp.exp(sink - top)
    weight = (probs / denom).astype(jnp.bfloat16)
    attended = jnp.einsum("nkgqs,nskd->nqkgd", weight, val_win, preferred_element_type=jnp.float32)
    return attended.astype(jnp.bfloat16).reshape(tokens, heads_local * HEAD)


MESH = pl.DeviceIdType.MESH
LANES = 128


def norm_rows(stream, gain, bias):
    mean = jnp.mean(stream, axis=-1, keepdims=True)
    spread = jnp.mean(jnp.square(stream - mean), axis=-1, keepdims=True)
    return (stream - mean) * lax.rsqrt(spread + norm_eps) * gain + bias


ROWS_Y, LAYERS, CORES, SIDES = 2, 4, 2, 2
PIECES = 2
ROW_PARTS = 2


def fits(tokens, up_weight):
    depth, hidden = up_weight.shape
    return (
        lax.axis_size("sp") == ROWS_Y * LAYERS
        and lax.axis_size("tp") == CORES * SIDES
        and depth % (2 * LANES) == 0
        and hidden % (2 * PIECES * LANES) == 0
        and tokens % (2 * WINDOW) == 0
        and tokens % (SIDES * CORES * ROW_PARTS * 32) == 0
    )


def block_kernel(
    n, m, q_ref, k_ref, v_ref, sinks_ref, slopes_ref, proj_ref, up_ref, down_ref, res_ref,
    gains_ref, biases_ref, out_ref,
    key_ext, val_ext, attended, att_in, proj_in, mix_out, mix_own, mix_in, up_all, down_all,
    normed_own, normed, act, terms, cross_in, joined, terms_in, total,
    tail_send, tail_recv, proj_send, proj_recv, att_send, att_recv, mix_send, mix_recv,
    main_send, extra_send, pass_send, z_recv, first_send, y_send, y_recv, all_send, all_recv,
    d_send, d_recv, row_send, row_recv, fwd_send, out_send, cross_send, cross_recv, join_send, out_recv,
):
    me, rank = lax.axis_index("sp"), lax.axis_index("tp")
    depth, hidden = up_ref.shape
    own_rows, width = res_ref.shape
    tokens = q_ref.shape[0]
    q_width = q_ref.shape[1]
    side_rows = tokens // SIDES
    y, z = lax.rem(me, ROWS_Y), lax.div(me, ROWS_Y)
    x, c = lax.div(rank, CORES), lax.rem(rank, CORES)
    half, zl = lax.div(z, 2), lax.rem(z, 2)
    oy, ox, oc = 1 - y, 1 - x, 1 - c
    oz = z + 1 - 2 * zl
    u = zl + half - 2 * zl * half
    step_rows = 32

    home = c == zl
    away = c != zl
    h1 = 1 - lax.rem(c + zl, 2)

    def layer(w):
        return w + half * (LAYERS - 1 - 2 * w)

    def source(k):
        return layer(u if k == 0 else 1 - u if k == 1 else k)

    def at(x_, y_, z_, c_):
        return (z_ * ROWS_Y + y_, x_ * CORES + c_)

    barrier = pltpu.get_barrier_semaphore()
    partners = [at(x, y, z, oc)]
    for k in range(1, LAYERS):
        for core in range(CORES):
            partners.append(at(x, y, lax.rem(z + k, LAYERS), core))
    for core in range(CORES):
        partners.append(at(x, oy, z, core))
        partners.append(at(ox, y, z, core))
    partners.append(at(x, oy, lax.rem(z + 2 * y - 1 + LAYERS, LAYERS), c))
    for there in partners:
        pl.semaphore_signal(barrier, inc=1, device_id=there, device_id_type=MESH)
    pl.semaphore_wait(barrier, len(partners))

    def remote(source, target, send, recv, device):
        return pltpu.make_async_remote_copy(
            src_ref=source, dst_ref=target, send_sem=send, recv_sem=recv,
            device_id=device, device_id_type=MESH,
        )

    def held(kind, s, h, p):
        if kind == 0:
            rows = depth // (2 * PIECES)
            off = s * depth + h * (depth // 2) + p * rows
            return up_all.at[pl.ds(pl.multiple_of(off, rows), rows)]
        rows = hidden // (2 * PIECES)
        off = h * (hidden // 2) + p * rows
        return down_all.at[s, pl.ds(pl.multiple_of(off, rows), rows)]

    def own_piece(kind, h, p):
        ref = up_ref if kind == 0 else down_ref
        rows = ref.shape[0] // (2 * PIECES)
        return ref.at[pl.ds(h * (ref.shape[0] // 2) + p * rows, rows)]

    w_main = h1 * (u + 2) + (1 - h1) * (u + 1)
    k_main = h1 * (3 - u) + (1 - h1) * (1 + u)

    def main(kind, h, p):
        return remote(
            own_piece(kind, h, p), held(kind, me, h, p), main_send.at[kind, h, p],
            z_recv.at[kind, k_main, p], at(x, y, layer(w_main), h),
        )

    def extra(kind, h, p):
        return remote(
            own_piece(kind, h, p), held(kind, me, h, p), extra_send.at[kind, h, p],
            z_recv.at[kind, 1, p], at(x, y, layer(0), h),
        )

    extra_here = (u == 1) & away

    def column(k, other):
        return source(k) * ROWS_Y + (oy if other else y)

    def z_piece(kind, k, p):
        ref = held(kind, column(k, 0), c, p)
        return remote(ref, ref, pass_send.at[kind, p], z_recv.at[kind, k, p], at(x, y, z, oc))

    def passed(kind, p):
        ref = held(kind, column(1, 0), c, p)
        return remote(
            ref, ref, pass_send.at[kind, p], z_recv.at[kind, 3, p], at(x, y, layer(3), c)
        )

    def first(kind, h, p):
        return remote(
            own_piece(kind, h, p), held(kind, me, h, p), first_send.at[kind, h, p],
            y_recv.at[kind, 0, p], at(x, oy, z, h),
        )

    def y_out(kind, k, p):
        ref = held(kind, column(k, 0), c, p)
        return remote(
            ref, ref, y_send.at[kind, k, p], y_recv.at[kind, k, p], at(x, oy, z, c)
        )

    def y_in(kind, k, p):
        ref = held(kind, column(k, 1), c, p)
        return remote(
            ref, ref, y_send.at[kind, k, p], y_recv.at[kind, k, p], at(x, oy, z, c)
        )

    def across(kind, other, k, p, h):
        ref = held(kind, column(k, other), h, p)
        return remote(
            ref, ref, d_send.at[kind, other, k, p], d_recv.at[kind, other, k, p],
            at(x, y, z, oc),
        )

    def whole(kind):
        ref = up_ref if kind == 0 else down_ref
        if kind == 0:
            target = up_all.at[pl.ds(pl.multiple_of(me * depth, depth), depth)]
        else:
            target = down_all.at[me]
        return remote(ref, target, all_send.at[kind], all_recv.at[kind], at(x, y, z, oc))

    def launch_local(kind):
        @pl.when(home)
        def _():
            whole(kind).start()
            for p in range(PIECES):
                for h in range(2):
                    first(kind, h, p).start()

    def launch_main(kind):
        for p in range(PIECES):
            for h in range(2):
                main(kind, h, p).start()

    def launch_extra(kind):
        @pl.when(extra_here)
        def _():
            for p in range(PIECES):
                for h in range(2):
                    extra(kind, h, p).start()

    def serve_z(kind, k):
        for p in range(PIECES):
            z_piece(kind, k, p).wait_recv()
            if k == 1:
                @pl.when(u == 1)
                def _():
                    passed(kind, p).start()
            y_out(kind, k, p).start()
            across(kind, 0, k, p, c).start()

    def serve_y(kind, k):
        for p in range(PIECES):
            y_in(kind, k, p).wait_recv()
            across(kind, 1, k, p, c).start()

    def need(kind, other, k):
        if k == 0 and not other:
            @pl.when(away)
            def _():
                whole(kind).wait_recv()
            return
        for p in range(PIECES):
            across(kind, other, k, p, oc).wait_recv()

    after = lax.rem(me + 1, n)
    tails = [
        remote(
            ref.at[pl.ds(tokens - WINDOW, WINDOW)], ext.at[pl.ds(0, WINDOW)],
            tail_send.at[i], tail_recv.at[i], (after, rank),
        )
        for i, (ref, ext) in enumerate(((k_ref, key_ext), (v_ref, val_ext)))
    ]
    for copy in tails:
        copy.start()
    launch_main(0)
    launch_extra(0)
    proj_copy = remote(proj_ref, proj_in, proj_send.at[0], proj_recv.at[0], at(x, y, z, oc))
    proj_copy.start()
    launch_local(0)
    key_ext[WINDOW:] = k_ref[...]
    val_ext[WINDOW:] = v_ref[...]

    @pl.when(home)
    def _():
        up_all[pl.ds(pl.multiple_of(me * depth, depth), depth)] = up_ref[...]
        down_all[me] = down_ref[...]

    for copy in tails:
        copy.wait_recv()

    blocks = tokens // WINDOW
    heads_local = q_width // HEAD
    group = heads_local // (k_ref.shape[1] // HEAD)

    def windows(first_block, count):
        @pl.loop(0, count)
        def _(i):
            start = pl.multiple_of((first_block + i) * WINDOW, WINDOW)
            rows, span = pl.ds(start, WINDOW), pl.ds(start, 2 * WINDOW)
            q_index = lax.broadcasted_iota(jnp.int32, (WINDOW, 2 * WINDOW), 0)
            k_index = lax.broadcasted_iota(jnp.int32, (WINDOW, 2 * WINDOW), 1)
            dist = q_index + WINDOW - k_index
            key_pos = me * tokens + start - WINDOW + k_index
            valid = (dist >= 0) & (dist < WINDOW) & (key_pos >= 0)
            far = dist.astype(jnp.float32)
            for h in range(heads_local):
                columns = slice(h * HEAD, (h + 1) * HEAD)
                shared = slice(h // group * HEAD, (h // group + 1) * HEAD)
                logits = lax.dot_general(
                    q_ref[rows, columns], key_ext[span, shared], (((1,), (1,)), ((), ())),
                    preferred_element_type=jnp.float32,
                ) * HEAD ** (-0.5)
                logits = jnp.where(valid, logits - slopes_ref[h] * far, neg_big)
                sink = sinks_ref[h]
                top = jnp.maximum(jnp.max(logits, axis=-1, keepdims=True), sink)
                probs = jnp.exp(logits - top)
                denom = jnp.sum(probs, axis=-1, keepdims=True) + jnp.exp(sink - top)
                weight = (probs / denom).astype(jnp.bfloat16)
                attended[rows, columns] = jnp.dot(
                    weight, val_ext[span, shared], preferred_element_type=jnp.float32
                ).astype(jnp.bfloat16)

    def rows_of(side, core):
        start = side * side_rows + core * own_rows
        return pl.ds(pl.multiple_of(start, own_rows), own_rows)

    def swap(i, side):
        return remote(
            attended.at[rows_of(side, oc)], att_in.at[i], att_send.at[i], att_recv.at[i],
            at(x, y, z, oc),
        )

    tile = 2 * LANES

    def project(i, side, target):
        @pl.loop(0, width // tile)
        def _(j):
            columns = pl.ds(pl.multiple_of(j * tile, tile), tile)
            target[:, columns] = (
                jnp.dot(
                    attended[rows_of(side, c)], proj_ref[:, columns],
                    preferred_element_type=jnp.float32,
                )
                + jnp.dot(att_in[i], proj_in[:, columns], preferred_element_type=jnp.float32)
            ).astype(target.dtype)

    part_rows = own_rows // ROW_PARTS

    def mix_copy(p):
        rows = pl.ds(p * part_rows, part_rows)
        return remote(
            mix_out.at[rows], mix_in.at[rows], mix_send.at[p], mix_recv.at[p], at(ox, y, z, c)
        )

    windows(ox * (blocks // 2), blocks // 2)
    swap(0, ox).start()
    proj_copy.wait_recv()
    swap(0, ox).wait_recv()
    project(0, ox, mix_out)
    for p in range(ROW_PARTS):
        mix_copy(p).start()
    serve_y(0, 0)
    windows(x * (blocks // 2), blocks // 2)
    swap(1, x).start()
    serve_z(0, 1)
    swap(1, x).wait_recv()
    project(1, x, mix_own)
    serve_y(0, 1)

    def rank_rows(r, p):
        start = r * own_rows + p * part_rows
        return pl.ds(pl.multiple_of(start, part_rows), part_rows)

    def row_copy(t, p):
        source_ref, rows = normed_own.at[pl.ds(p * part_rows, part_rows)], rank_rows(rank, p)
        there = [at(x, y, z, oc), at(ox, y, z, zl), at(x, y, oz, zl)][t]
        return remote(
            source_ref, normed.at[rows], row_send.at[t, p], row_recv.at[rank, p], there
        )

    def row_in(side, core, p):
        r = side * CORES + core
        ref = normed.at[rank_rows(r, p)]
        return remote(ref, ref, fwd_send.at[core, p], row_recv.at[r, p], at(ox, y, z, c))

    for p in range(ROW_PARTS):
        mix_copy(p).wait_recv()

        @pl.loop(0, part_rows // step_rows)
        def _(i):
            start = pl.multiple_of(p * part_rows + i * step_rows, step_rows)
            rows = pl.ds(start, step_rows)
            mix = mix_own[rows] + mix_in[rows].astype(jnp.float32)
            stream = deep_alpha * res_ref[rows].astype(jnp.float32) + mix
            made = norm_rows(stream, gains_ref[0:1], biases_ref[0:1]).astype(jnp.bfloat16)
            normed_own[rows] = made

            @pl.when(home)
            def _():
                mine = pl.ds(pl.multiple_of(rank * own_rows + start, step_rows), step_rows)
                normed[mine] = made

        row_copy(2, p).start()
        row_copy(1, p).start()

        @pl.when(away)
        def _():
            row_copy(0, p).start()

    serve_z(0, 2)
    launch_main(1)
    launch_extra(1)
    launch_local(1)
    serve_y(0, 2)

    @pl.when(away)
    def _():
        for p in range(ROW_PARTS):
            for core in range(CORES):
                row_in(x, core, p).wait_recv()
                row_in(x, core, p).start()

    serve_z(0, 3)
    serve_y(0, 3)
    serve_z(1, 1)
    for k in range(LAYERS):
        for other in range(2):
            need(0, other, k)

    for p in range(ROW_PARTS):
        for core in range(CORES):
            row_in(ox, core, p).wait_recv()

        @pl.when(home)
        def _():
            row_in(x, oc, p).wait_recv()

    tiles = hidden // tile

    def upward(first, last):
        @pl.loop(first, last)
        def _(i):
            columns = pl.ds(pl.multiple_of(i * tile, tile), tile)
            made = jnp.dot(normed[...], up_all[:, columns], preferred_element_type=jnp.float32)
            act[:, columns] = jnp.square(jnp.maximum(made, 0.0)).astype(jnp.bfloat16)

    parts = 4
    for part in range(parts):
        upward(part * tiles // parts, (part + 1) * tiles // parts)
        if part == 0:
            serve_y(1, 0)
        elif part == 1:
            serve_y(1, 1)
        elif part == 2:
            serve_z(1, 2)
        else:
            serve_y(1, 2)

    steps = 2 * LAYERS

    def out_copy(i, t):
        r = [x * CORES + oc, ox * CORES, ox * CORES + 1][t]
        rows = pl.ds(pl.multiple_of(r * own_rows, own_rows), own_rows)
        there = [at(x, y, z, oc), at(ox, y, z, 0), at(ox, y, z, 1)][t]
        slot = 0 if t == 0 else 1
        return remote(
            terms.at[i, rows], terms_in.at[slot, i], out_send.at[i, t], out_recv.at[slot, i], there
        )

    def cross_copy(i):
        rows = pl.ds(pl.multiple_of(ox * side_rows, side_rows), side_rows)
        return remote(
            terms.at[i, rows], cross_in.at[i], cross_send.at[i], cross_recv.at[i], at(ox, y, z, c)
        )

    def join_copy(i, core):
        return remote(
            joined.at[i, pl.ds(core * own_rows, own_rows)], terms_in.at[2, i],
            join_send.at[i, core], out_recv.at[2, i], at(x, y, oz, core),
        )

    held_rows = pl.ds(pl.multiple_of(rank * own_rows, own_rows), own_rows)

    def downward(i):
        s = column(i // 2, i % 2)
        terms[i] = jnp.dot(
            act[...], down_all[s], preferred_element_type=jnp.float32
        ).astype(jnp.bfloat16)

        @pl.when(home)
        def _():
            for t in range(3):
                out_copy(i, t).start()
            terms_in[0, i] = terms[i, held_rows]

        @pl.when(away)
        def _():
            cross_copy(i).start()

    def join(i):
        @pl.when(away)
        def _():
            cross_copy(i).wait_recv()
            rows = pl.ds(pl.multiple_of(x * side_rows, side_rows), side_rows)
            joined[i] = (
                terms[i, rows].astype(jnp.float32) + cross_in[i].astype(jnp.float32)
            ).astype(jnp.bfloat16)
            for core in range(CORES):
                join_copy(i, core).start()

    def collect(k):
        for other in range(2):
            i = 2 * k + other
            i2 = 2 * (1 - k if k < 2 else k) + other

            @pl.when(away)
            def _():
                out_copy(i, 0).wait_recv()

            out_copy(i, 1).wait_recv()
            join_copy(i2, 0).wait_recv()
            columns = pl.ds(pl.multiple_of(column(k, other) * depth, depth), depth)
            block = terms_in[0, i].astype(jnp.float32)
            block += terms_in[1, i].astype(jnp.float32)
            block += terms_in[2, i2].astype(jnp.float32)
            total[:, columns] = deep_alpha * normed_own[:, columns].astype(jnp.float32) + block

    for i in range(steps):
        k, other = i // 2, i % 2
        if i == 6:
            serve_z(1, 3)
        if i == 7:
            serve_y(1, 3)
        need(1, other, k)
        downward(i)
        if i >= 1:
            join(i - 1)
        if i == 4:
            collect(0)
        if i == 5:
            collect(1)
    join(steps - 1)
    collect(2)
    collect(3)

    @pl.loop(0, own_rows // step_rows)
    def _(i):
        rows = pl.ds(pl.multiple_of(i * step_rows, step_rows), step_rows)
        out_ref[rows] = norm_rows(total[rows], gains_ref[1:2], biases_ref[1:2]).astype(jnp.bfloat16)

    for copy in tails:
        copy.wait_send()
    proj_copy.wait_send()
    swap(0, ox).wait_send()
    swap(1, x).wait_send()
    for p in range(ROW_PARTS):
        mix_copy(p).wait_send()
        row_copy(1, p).wait_send()
        row_copy(2, p).wait_send()
    for kind in range(2):
        for p in range(PIECES):
            for h in range(2):
                main(kind, h, p).wait_send()
            for k in range(LAYERS):
                if k > 0:
                    y_out(kind, k, p).wait_send()
                    across(kind, 0, k, p, c).wait_send()
                across(kind, 1, k, p, c).wait_send()

    @pl.when(extra_here)
    def _():
        for kind in range(2):
            for p in range(PIECES):
                for h in range(2):
                    extra(kind, h, p).wait_send()

    @pl.when(u == 1)
    def _():
        for kind in range(2):
            for p in range(PIECES):
                passed(kind, p).wait_send()

    @pl.when(home)
    def _():
        for kind in range(2):
            whole(kind).wait_send()
            for p in range(PIECES):
                for h in range(2):
                    first(kind, h, p).wait_send()
        for i in range(steps):
            for t in range(3):
                out_copy(i, t).wait_send()

    @pl.when(away)
    def _():
        for p in range(ROW_PARTS):
            row_copy(0, p).wait_send()
            for core in range(CORES):
                row_in(x, core, p).wait_send()
        for i in range(steps):
            cross_copy(i).wait_send()
            for core in range(CORES):
                join_copy(i, core).wait_send()


def fused_block(
    queries, keys, values, sinks, slopes, out_weight, up_weight, down_weight, residual, gains, biases
):
    n, m = lax.axis_size("sp"), lax.axis_size("tp")
    depth, hidden = up_weight.shape
    tokens = queries.shape[0]
    own_rows, width = residual.shape
    side_rows, steps = tokens // SIDES, 2 * LAYERS
    vmem, smem = pl.BlockSpec(memory_space=pltpu.VMEM), pl.BlockSpec(memory_space=pltpu.SMEM)
    bf16, dma = jnp.bfloat16, pltpu.SemaphoreType.DMA
    return pl.pallas_call(
        functools.partial(block_kernel, n, m),
        out_shape=jax.ShapeDtypeStruct(residual.shape, bf16),
        in_specs=[vmem] * 3 + [smem] * 2 + [vmem] * 6,
        out_specs=pl.BlockSpec(memory_space=pltpu.VMEM),
        scratch_shapes=[
            pltpu.VMEM((tokens + WINDOW, keys.shape[1]), bf16),
            pltpu.VMEM((tokens + WINDOW, keys.shape[1]), bf16),
            pltpu.VMEM(queries.shape, bf16),
            pltpu.VMEM((SIDES, own_rows, queries.shape[1]), bf16),
            pltpu.VMEM(out_weight.shape, bf16),
            pltpu.VMEM((own_rows, width), bf16),
            pltpu.VMEM((own_rows, width), jnp.float32),
            pltpu.VMEM((own_rows, width), bf16),
            pltpu.VMEM((width, hidden), bf16),
            pltpu.VMEM((n, hidden, depth), bf16),
            pltpu.VMEM((own_rows, width), bf16),
            pltpu.VMEM((tokens, width), bf16),
            pltpu.VMEM((tokens, hidden), bf16),
            pltpu.VMEM((steps, tokens, depth), bf16),
            pltpu.VMEM((steps, side_rows, depth), bf16),
            pltpu.VMEM((steps, side_rows, depth), bf16),
            pltpu.VMEM((3, steps, own_rows, depth), bf16),
            pltpu.VMEM((own_rows, width), jnp.float32),
            dma((2,)),
            dma((2,)),
            dma((1,)),
            dma((1,)),
            dma((SIDES,)),
            dma((SIDES,)),
            dma((ROW_PARTS,)),
            dma((ROW_PARTS,)),
            dma((2, 2, PIECES)),
            dma((2, 2, PIECES)),
            dma((2, PIECES)),
            dma((2, LAYERS, PIECES)),
            dma((2, 2, PIECES)),
            dma((2, LAYERS, PIECES)),
            dma((2, LAYERS, PIECES)),
            dma((2,)),
            dma((2,)),
            dma((2, 2, LAYERS, PIECES)),
            dma((2, 2, LAYERS, PIECES)),
            dma((3, ROW_PARTS)),
            dma((m, ROW_PARTS)),
            dma((CORES, ROW_PARTS)),
            dma((steps, 3)),
            dma((steps,)),
            dma((steps,)),
            dma((steps, CORES)),
            dma((3, steps)),
        ],
        compiler_params=pltpu.CompilerParams(
            collective_id=0, has_side_effects=True, vmem_limit_bytes=60 * 1024 * 1024
        ),
    )(
        queries, keys, values, sinks, slopes, out_weight, up_weight, down_weight, residual, gains,
        biases,
    )


def on_device(
    queries, keys, values, residual, sinks, out_weight, up_weight, down_weight, gains, biases
):
    tokens = queries.shape[0]
    rank_tp = lax.axis_index("tp")
    if fits(tokens, up_weight):
        heads_local = sinks.shape[0]
        heads = (jnp.arange(heads_local, dtype=jnp.int32) + rank_tp * heads_local).astype(jnp.float32)
        slopes = jnp.exp2(-8.0 * (heads + 1.0) / HEADS)
        return fused_block(
            queries, keys, values, sinks, slopes, out_weight, up_weight, down_weight, residual,
            gains, biases,
        )
    tails = jnp.stack([keys[tokens - WINDOW :], values[tokens - WINDOW :]])
    before = from_behind(tails, "sp", 1)
    offset = lax.axis_index("sp") * tokens
    attended = attend(queries, keys, values, before, sinks, offset, rank_tp)
    part = jnp.dot(attended, out_weight, preferred_element_type=jnp.float32).astype(jnp.bfloat16)
    up_full, down_full = (
        lax.all_gather(up_weight, "sp", axis=0, tiled=True),
        lax.all_gather(down_weight, "sp", axis=1, tiled=True),
    )
    mix = lax.psum_scatter(
        part,
        "tp",
        scatter_dimension=0,
        tiled=True,
    ).astype(jnp.float32)
    normed = layer_norm(deep_alpha * residual.astype(jnp.float32) + mix, gains[0], biases[0])
    whole = lax.all_gather(normed, "tp", axis=0, tiled=True)
    upward = jnp.dot(whole, up_full, preferred_element_type=jnp.float32)
    act = jnp.square(jax.nn.relu(upward)).astype(jnp.bfloat16)
    terms = jnp.dot(act, down_full, preferred_element_type=jnp.float32)
    ffn = lax.psum_scatter(
        terms.astype(jnp.bfloat16), "tp", scatter_dimension=0, tiled=True
    ).astype(jnp.float32)
    return layer_norm(deep_alpha * normed.astype(jnp.float32) + ffn, gains[1], biases[1])


def solution(mesh):
    return jax.shard_map(
        on_device,
        mesh=mesh,
        in_specs=(
            P("sp", "tp"),
            P("sp", "tp"),
            P("sp", "tp"),
            P(("sp", "tp"), None),
            P("tp"),
            P("tp", None),
            P("sp", "tp"),
            P("tp", "sp"),
            P(),
            P(),
        ),
        out_specs=P(("sp", "tp"), None),
        check_vma=False,
    )
```

```python
import functools

import jax
import jax.numpy as jnp
from jax import lax
from jax.experimental import pallas as pl
from jax.experimental.pallas import tpu as pltpu
from jax.sharding import PartitionSpec as P

HEADS = 12
HEAD = 128
WINDOW = 128


deep_alpha = 1.6817928
norm_eps = 1e-05
neg_big = -1e30


def from_behind(block, axis, distance):
    devices = range(lax.axis_size(axis))
    route = [(i - distance, i) for i in devices if i - distance in devices]
    return lax.ppermute(block, axis, route)


def layer_norm(stream, gain, bias):
    mean = jnp.mean(stream, axis=-1, keepdims=True)
    spread = jnp.mean(jnp.square(stream - mean), axis=-1, keepdims=True)
    return ((stream - mean) * lax.rsqrt(spread + norm_eps) * gain + bias).astype(jnp.bfloat16)


def attend(queries, keys, values, before, sinks, offset, rank_tp):
    tokens = keys.shape[0]
    kv_local = keys.shape[1] // HEAD
    heads_local = sinks.shape[0]
    group = heads_local // kv_local
    blocks = tokens // WINDOW
    q_blocks = queries.reshape(blocks, WINDOW, kv_local, group, HEAD)
    key_ext = jnp.concatenate([before[0], keys], axis=0).reshape(tokens + WINDOW, kv_local, HEAD)
    val_ext = jnp.concatenate([before[1], values], axis=0).reshape(tokens + WINDOW, kv_local, HEAD)
    key_win = jnp.concatenate(
        [
            key_ext[:tokens].reshape(blocks, WINDOW, kv_local, HEAD),
            key_ext[WINDOW:].reshape(blocks, WINDOW, kv_local, HEAD),
        ],
        axis=1,
    )
    val_win = jnp.concatenate(
        [
            val_ext[:tokens].reshape(blocks, WINDOW, kv_local, HEAD),
            val_ext[WINDOW:].reshape(blocks, WINDOW, kv_local, HEAD),
        ],
        axis=1,
    )
    logits = jnp.einsum(
        "nqkgd,nskd->nkgqs", q_blocks, key_win, preferred_element_type=jnp.float32
    ) * HEAD ** (-0.5)
    q_index = jnp.arange(WINDOW, dtype=jnp.int32)[:, None]
    k_index = jnp.arange(2 * WINDOW, dtype=jnp.int32)[None, :]
    dist = q_index + WINDOW - k_index
    block_id = jnp.arange(blocks, dtype=jnp.int32)[:, None, None]
    key_pos = offset + block_id * WINDOW - WINDOW + k_index
    valid = (dist >= 0) & (dist < WINDOW) & (key_pos >= 0)
    heads = (jnp.arange(heads_local, dtype=jnp.int32) + rank_tp * heads_local).astype(jnp.float32)
    slopes = jnp.exp2(-8.0 * (heads + 1.0) / HEADS).reshape(kv_local, group)[:, :, None, None]
    logits = logits - slopes * dist.astype(jnp.float32)
    logits = jnp.where(valid[:, None, None], logits, neg_big)
    sink = sinks.reshape(kv_local, group)[:, :, None, None]
    top = jnp.maximum(jnp.max(logits, axis=-1, keepdims=True), sink)
    probs = jnp.exp(logits - top)
    denom = jnp.sum(probs, axis=-1, keepdims=True) + jnp.exp(sink - top)
    weight = (probs / denom).astype(jnp.bfloat16)
    attended = jnp.einsum("nkgqs,nskd->nqkgd", weight, val_win, preferred_element_type=jnp.float32)
    return attended.astype(jnp.bfloat16).reshape(tokens, heads_local * HEAD)


MESH = pl.DeviceIdType.MESH
LANES = 128


def norm_rows(stream, gain, bias):
    mean = jnp.mean(stream, axis=-1, keepdims=True)
    spread = jnp.mean(jnp.square(stream - mean), axis=-1, keepdims=True)
    return (stream - mean) * lax.rsqrt(spread + norm_eps) * gain + bias


ROWS_Y, LAYERS, CORES, SIDES = 2, 4, 2, 2
PIECES = 1
ROW_PARTS = 2


def fits(tokens, up_weight):
    depth, hidden = up_weight.shape
    return (
        lax.axis_size("sp") == ROWS_Y * LAYERS
        and lax.axis_size("tp") == CORES * SIDES
        and depth % (2 * LANES) == 0
        and hidden % (2 * PIECES * LANES) == 0
        and tokens % (2 * WINDOW) == 0
        and tokens % (SIDES * CORES * ROW_PARTS * 32) == 0
    )


def block_kernel(
    n, m, q_ref, k_ref, v_ref, sinks_ref, gains_ref, biases_ref, proj_hbm, up_ref, down_ref, res_hbm, out_ref,
    key_ext, val_ext, proj_ref, res_ref, attended, att_in, proj_in, mix_out, mix_own, mix_in, up_all, down_all,
    normed_own, normed, act, terms, cross_in, joined, terms_in, total,
    tail_send, tail_recv, proj_send, proj_recv, att_send, att_recv, mix_send, mix_recv,
    main_send, extra_send, pass_send, z_recv, first_send, y_send, y_recv, all_send, all_recv,
    d_send, d_recv, row_send, row_recv, fwd_send, out_send, cross_send, cross_recv, join_send, out_recv, local_sem,
):
    me, rank = lax.axis_index("sp"), lax.axis_index("tp")
    depth, hidden = up_ref.shape
    own_rows, width = res_ref.shape
    tokens = q_ref.shape[0]
    q_width = q_ref.shape[1]
    side_rows = tokens // SIDES
    y, z = lax.rem(me, ROWS_Y), lax.div(me, ROWS_Y)
    x, c = lax.div(rank, CORES), lax.rem(rank, CORES)
    half, zl = lax.div(z, 2), lax.rem(z, 2)
    oy, ox, oc = 1 - y, 1 - x, 1 - c
    oz = z + 1 - 2 * zl
    u = zl + half - 2 * zl * half
    step_rows = 32

    home = c == zl
    away = c != zl
    h1 = 1 - lax.rem(c + zl, 2)

    def layer(w):
        return w + half * (LAYERS - 1 - 2 * w)

    def source(k):
        return layer(u if k == 0 else 1 - u if k == 1 else k)

    def at(x_, y_, z_, c_):
        return (z_ * ROWS_Y + y_, x_ * CORES + c_)

    barrier = pltpu.get_barrier_semaphore()
    partners = [at(x, y, z, oc)]
    for k in range(1, LAYERS):
        for core in range(CORES):
            partners.append(at(x, y, lax.rem(z + k, LAYERS), core))
    for core in range(CORES):
        partners.append(at(x, oy, z, core))
        partners.append(at(ox, y, z, core))
    partners.append(at(x, oy, lax.rem(z + 2 * y - 1 + LAYERS, LAYERS), c))
    for there in partners:
        pl.semaphore_signal(barrier, inc=1, device_id=there, device_id_type=MESH)
    pl.semaphore_wait(barrier, len(partners))

    def remote(source, target, send, recv, device):
        return pltpu.make_async_remote_copy(
            src_ref=source, dst_ref=target, send_sem=send, recv_sem=recv,
            device_id=device, device_id_type=MESH,
        )

    def held(kind, s, h, p):
        if kind == 0:
            rows = depth // (2 * PIECES)
            off = s * depth + h * (depth // 2) + p * rows
            return up_all.at[pl.ds(pl.multiple_of(off, rows), rows)]
        rows = hidden // (2 * PIECES)
        off = h * (hidden // 2) + p * rows
        return down_all.at[s, pl.ds(pl.multiple_of(off, rows), rows)]

    def own_piece(kind, h, p):
        ref = up_ref if kind == 0 else down_ref
        rows = ref.shape[0] // (2 * PIECES)
        return ref.at[pl.ds(h * (ref.shape[0] // 2) + p * rows, rows)]

    w_main = h1 * (u + 2) + (1 - h1) * (u + 1)
    k_main = h1 * (3 - u) + (1 - h1) * (1 + u)

    def main(kind, h, p):
        return remote(
            own_piece(kind, h, p), held(kind, me, h, p), main_send.at[kind, h, p],
            z_recv.at[kind, k_main, p], at(x, y, layer(w_main), h),
        )

    def extra(kind, h, p):
        return remote(
            own_piece(kind, h, p), held(kind, me, h, p), extra_send.at[kind, h, p],
            z_recv.at[kind, 1, p], at(x, y, layer(0), h),
        )

    extra_here = (u == 1) & away

    def column(k, other):
        return source(k) * ROWS_Y + (oy if other else y)

    def z_piece(kind, k, p):
        ref = held(kind, column(k, 0), c, p)
        return remote(ref, ref, pass_send.at[kind, p], z_recv.at[kind, k, p], at(x, y, z, oc))

    def passed(kind, p):
        ref = held(kind, column(1, 0), c, p)
        return remote(
            ref, ref, pass_send.at[kind, p], z_recv.at[kind, 3, p], at(x, y, layer(3), c)
        )

    def first(kind, h, p):
        return remote(
            own_piece(kind, h, p), held(kind, me, h, p), first_send.at[kind, h, p],
            y_recv.at[kind, 0, p], at(x, oy, z, h),
        )

    def y_out(kind, k, p):
        ref = held(kind, column(k, 0), c, p)
        return remote(
            ref, ref, y_send.at[kind, k, p], y_recv.at[kind, k, p], at(x, oy, z, c)
        )

    def y_in(kind, k, p):
        ref = held(kind, column(k, 1), c, p)
        return remote(
            ref, ref, y_send.at[kind, k, p], y_recv.at[kind, k, p], at(x, oy, z, c)
        )

    def across(kind, other, k, p, h):
        ref = held(kind, column(k, other), h, p)
        return remote(
            ref, ref, d_send.at[kind, other, k, p], d_recv.at[kind, other, k, p],
            at(x, y, z, oc),
        )

    def whole(kind):
        ref = up_ref if kind == 0 else down_ref
        if kind == 0:
            target = up_all.at[pl.ds(pl.multiple_of(me * depth, depth), depth)]
        else:
            target = down_all.at[me]
        return remote(ref, target, all_send.at[kind], all_recv.at[kind], at(x, y, z, oc))

    def launch_local(kind):
        @pl.when(home)
        def _():
            whole(kind).start()
            for p in range(PIECES):
                for h in range(2):
                    first(kind, h, p).start()

    def launch_main(kind):
        for p in range(PIECES):
            for h in range(2):
                main(kind, h, p).start()

    def launch_extra(kind):
        @pl.when(extra_here)
        def _():
            for p in range(PIECES):
                for h in range(2):
                    extra(kind, h, p).start()

    def serve_z(kind, k):
        for p in range(PIECES):
            z_piece(kind, k, p).wait_recv()
            if k == 1:
                @pl.when(u == 1)
                def _():
                    passed(kind, p).start()
            y_out(kind, k, p).start()
            across(kind, 0, k, p, c).start()

    def serve_y(kind, k):
        for p in range(PIECES):
            y_in(kind, k, p).wait_recv()
            across(kind, 1, k, p, c).start()

    def need(kind, other, k):
        if k == 0 and not other:
            @pl.when(away)
            def _():
                whole(kind).wait_recv()

            @pl.when(home)
            def _():
                own_block(kind).wait()
            return
        for p in range(PIECES):
            across(kind, other, k, p, oc).wait_recv()

    after = lax.rem(me + 1, n)
    tails = [
        remote(
            ref.at[pl.ds(tokens - WINDOW, WINDOW)], ext.at[pl.ds(0, WINDOW)],
            tail_send.at[i], tail_recv.at[i], (after, rank),
        )
        for i, (ref, ext) in enumerate(((k_ref, key_ext), (v_ref, val_ext)))
    ]
    for copy in tails:
        copy.start()
    launch_main(0)
    launch_extra(0)
    proj_copy = remote(proj_hbm, proj_in, proj_send.at[0], proj_recv.at[0], at(x, y, z, oc))
    proj_copy.start()
    launch_local(0)
    proj_local = pltpu.make_async_copy(proj_hbm, proj_ref, local_sem.at[0])
    res_local = pltpu.make_async_copy(res_hbm, res_ref, local_sem.at[1])
    proj_local.start()
    res_local.start()

    def own_block(kind):
        if kind == 0:
            target = up_all.at[pl.ds(pl.multiple_of(me * depth, depth), depth)]
            return pltpu.make_async_copy(up_ref, target, local_sem.at[2])
        return pltpu.make_async_copy(down_ref, down_all.at[me], local_sem.at[3])

    @pl.when(home)
    def _():
        own_block(0).start()
        own_block(1).start()

    key_ext[WINDOW:] = k_ref[...]
    val_ext[WINDOW:] = v_ref[...]

    blocks = tokens // WINDOW
    heads_local = q_width // HEAD
    group = heads_local // (k_ref.shape[1] // HEAD)

    slopes = [
        jnp.exp2(
            jnp.full((1, 2 * WINDOW), -8.0 / HEADS, jnp.float32)
            * (rank * heads_local + (h + 1)).astype(jnp.float32)
        )
        for h in range(heads_local)
    ]

    def windows(first_block, count):
        @pl.loop(0, count)
        def _(i):
            start = pl.multiple_of((first_block + i) * WINDOW, WINDOW)
            rows, span = pl.ds(start, WINDOW), pl.ds(start, 2 * WINDOW)
            q_index = lax.broadcasted_iota(jnp.int32, (WINDOW, 2 * WINDOW), 0)
            k_index = lax.broadcasted_iota(jnp.int32, (WINDOW, 2 * WINDOW), 1)
            dist = q_index + WINDOW - k_index
            key_pos = me * tokens + start - WINDOW + k_index
            valid = (dist >= 0) & (dist < WINDOW) & (key_pos >= 0)
            far = dist.astype(jnp.float32)
            for h in range(heads_local):
                columns = slice(h * HEAD, (h + 1) * HEAD)
                shared = slice(h // group * HEAD, (h // group + 1) * HEAD)
                logits = lax.dot_general(
                    q_ref[rows, columns], key_ext[span, shared], (((1,), (1,)), ((), ())),
                    preferred_element_type=jnp.float32,
                ) * HEAD ** (-0.5)
                logits = jnp.where(valid, logits - slopes[h] * far, neg_big)
                sink = sinks_ref[h]
                top = jnp.maximum(jnp.max(logits, axis=-1, keepdims=True), sink)
                probs = jnp.exp(logits - top)
                denom = jnp.sum(probs, axis=-1, keepdims=True) + jnp.exp(sink - top)
                weight = (probs / denom).astype(jnp.bfloat16)
                attended[rows, columns] = jnp.dot(
                    weight, val_ext[span, shared], preferred_element_type=jnp.float32
                ).astype(jnp.bfloat16)

    def rows_of(side, core):
        start = side * side_rows + core * own_rows
        return pl.ds(pl.multiple_of(start, own_rows), own_rows)

    def swap(i, side):
        return remote(
            attended.at[rows_of(side, oc)], att_in.at[i], att_send.at[i], att_recv.at[i],
            at(x, y, z, oc),
        )

    tile = 2 * LANES

    def project(i, side, target):
        @pl.loop(0, width // tile)
        def _(j):
            columns = pl.ds(pl.multiple_of(j * tile, tile), tile)
            target[:, columns] = (
                jnp.dot(
                    attended[rows_of(side, c)], proj_ref[:, columns],
                    preferred_element_type=jnp.float32,
                )
                + jnp.dot(att_in[i], proj_in[:, columns], preferred_element_type=jnp.float32)
            ).astype(target.dtype)

    part_rows = own_rows // ROW_PARTS

    def mix_copy(p):
        rows = pl.ds(p * part_rows, part_rows)
        return remote(
            mix_out.at[rows], mix_in.at[rows], mix_send.at[p], mix_recv.at[p], at(ox, y, z, c)
        )

    windows(ox * (blocks // 2) + 1, blocks // 2 - 1)
    for copy in tails:
        copy.wait_recv()
    windows(ox * (blocks // 2), 1)
    swap(0, ox).start()
    proj_local.wait()
    proj_copy.wait_recv()
    swap(0, ox).wait_recv()
    project(0, ox, mix_out)
    for p in range(ROW_PARTS):
        mix_copy(p).start()
    windows(x * (blocks // 2), blocks // 2)
    swap(1, x).start()
    serve_z(0, 1)
    swap(1, x).wait_recv()
    project(1, x, mix_own)
    res_local.wait()

    def rank_rows(r, p):
        start = r * own_rows + p * part_rows
        return pl.ds(pl.multiple_of(start, part_rows), part_rows)

    def row_copy(t, p):
        source_ref, rows = normed_own.at[pl.ds(p * part_rows, part_rows)], rank_rows(rank, p)
        there = [at(x, y, z, oc), at(ox, y, z, zl), at(x, y, oz, zl)][t]
        return remote(
            source_ref, normed.at[rows], row_send.at[t, p], row_recv.at[rank, p], there
        )

    def row_in(side, core, p):
        r = side * CORES + core
        ref = normed.at[rank_rows(r, p)]
        return remote(ref, ref, fwd_send.at[core, p], row_recv.at[r, p], at(ox, y, z, c))

    for p in range(ROW_PARTS):
        mix_copy(p).wait_recv()

        @pl.loop(0, part_rows // step_rows)
        def _(i):
            start = pl.multiple_of(p * part_rows + i * step_rows, step_rows)
            rows = pl.ds(start, step_rows)
            mix = mix_own[rows] + mix_in[rows].astype(jnp.float32)
            stream = deep_alpha * res_ref[rows].astype(jnp.float32) + mix
            made = norm_rows(stream, gains_ref[0:1], biases_ref[0:1]).astype(jnp.bfloat16)
            normed_own[rows] = made

            @pl.when(home)
            def _():
                mine = pl.ds(pl.multiple_of(rank * own_rows + start, step_rows), step_rows)
                normed[mine] = made

        row_copy(2, p).start()
        row_copy(1, p).start()

        @pl.when(away)
        def _():
            row_copy(0, p).start()

    serve_z(0, 2)

    @pl.when((u == 0) & away)
    def _():
        launch_main(1)

    serve_y(0, 0)
    serve_y(0, 1)

    serve_z(0, 3)

    @pl.when(((u == 1) & away) | ((u == 0) & home))
    def _():
        launch_main(1)

    launch_local(1)

    @pl.when(away)
    def _():
        for p in range(ROW_PARTS):
            for core in range(CORES):
                row_in(x, core, p).wait_recv()
                row_in(x, core, p).start()

    launch_extra(1)
    serve_y(0, 2)
    serve_y(0, 3)
    for k in range(LAYERS):
        for other in range(2):
            need(0, other, k)

    for p in range(ROW_PARTS):
        for core in range(CORES):
            row_in(ox, core, p).wait_recv()

        @pl.when(home)
        def _():
            row_in(x, oc, p).wait_recv()

    tiles = hidden // tile

    def upward(first, last):
        @pl.loop(first, last)
        def _(i):
            columns = pl.ds(pl.multiple_of(i * tile, tile), tile)
            made = jnp.dot(normed[...], up_all[:, columns], preferred_element_type=jnp.float32)
            act[:, columns] = jnp.square(jnp.maximum(made, 0.0)).astype(jnp.bfloat16)

    parts = 4
    for part in range(parts):
        upward(part * tiles // parts, (part + 1) * tiles // parts)
        if part == 0:
            @pl.when((u == 1) & home)
            def _():
                launch_main(1)

            serve_z(1, 1)

    steps = 2 * LAYERS

    def out_copy(i, t):
        r = [x * CORES + oc, ox * CORES, ox * CORES + 1][t]
        rows = pl.ds(pl.multiple_of(r * own_rows, own_rows), own_rows)
        there = [at(x, y, z, oc), at(ox, y, z, 0), at(ox, y, z, 1)][t]
        slot = 0 if t == 0 else 1
        return remote(
            terms.at[i, rows], terms_in.at[slot, i], out_send.at[i, t], out_recv.at[slot, i], there
        )

    def cross_copy(i):
        rows = pl.ds(pl.multiple_of(ox * side_rows, side_rows), side_rows)
        return remote(
            terms.at[i, rows], cross_in.at[i], cross_send.at[i], cross_recv.at[i], at(ox, y, z, c)
        )

    def join_copy(i, core):
        return remote(
            joined.at[i, pl.ds(core * own_rows, own_rows)], terms_in.at[2, i],
            join_send.at[i, core], out_recv.at[2, i], at(x, y, oz, core),
        )

    held_rows = pl.ds(pl.multiple_of(rank * own_rows, own_rows), own_rows)

    def downward(i):
        s = column(i // 2, i % 2)
        terms[i] = jnp.dot(
            act[...], down_all[s], preferred_element_type=jnp.float32
        ).astype(jnp.bfloat16)

        @pl.when(home)
        def _():
            for t in range(3):
                out_copy(i, t).start()
            terms_in[0, i] = terms[i, held_rows]

        @pl.when(away)
        def _():
            cross_copy(i).start()

    def join(i):
        @pl.when(away)
        def _():
            cross_copy(i).wait_recv()
            rows = pl.ds(pl.multiple_of(x * side_rows, side_rows), side_rows)
            joined[i] = (
                terms[i, rows].astype(jnp.float32) + cross_in[i].astype(jnp.float32)
            ).astype(jnp.bfloat16)
            for core in range(CORES):
                join_copy(i, core).start()

    def collect(k):
        for other in range(2):
            i = 2 * k + other
            i2 = 2 * (1 - k if k < 2 else k) + other

            @pl.when(away)
            def _():
                out_copy(i, 0).wait_recv()

            out_copy(i, 1).wait_recv()
            join_copy(i2, 0).wait_recv()
            columns = pl.ds(pl.multiple_of(column(k, other) * depth, depth), depth)
            block = terms_in[0, i].astype(jnp.float32)
            block += terms_in[1, i].astype(jnp.float32)
            block += terms_in[2, i2].astype(jnp.float32)
            total[:, columns] = deep_alpha * normed_own[:, columns].astype(jnp.float32) + block

    before = {
        1: [(serve_y, 0)],
        3: [(serve_z, 2), (serve_y, 1)],
        5: [(serve_z, 3), (serve_y, 2)],
        7: [(serve_y, 3)],
    }
    for i in range(steps):
        k, other = i // 2, i % 2
        for serve, at_k in before.get(i, []):
            serve(1, at_k)
        need(1, other, k)
        downward(i)
        if i >= 1:
            join(i - 1)
    join(steps - 1)
    for k in range(LAYERS):
        collect(k)

    @pl.loop(0, own_rows // step_rows)
    def _(i):
        rows = pl.ds(pl.multiple_of(i * step_rows, step_rows), step_rows)
        out_ref[rows] = norm_rows(total[rows], gains_ref[1:2], biases_ref[1:2]).astype(jnp.bfloat16)

    for copy in tails:
        copy.wait_send()
    proj_copy.wait_send()
    swap(0, ox).wait_send()
    swap(1, x).wait_send()
    for p in range(ROW_PARTS):
        mix_copy(p).wait_send()
        row_copy(1, p).wait_send()
        row_copy(2, p).wait_send()
    for kind in range(2):
        for p in range(PIECES):
            for h in range(2):
                main(kind, h, p).wait_send()
            for k in range(LAYERS):
                if k > 0:
                    y_out(kind, k, p).wait_send()
                    across(kind, 0, k, p, c).wait_send()
                across(kind, 1, k, p, c).wait_send()

    @pl.when(extra_here)
    def _():
        for kind in range(2):
            for p in range(PIECES):
                for h in range(2):
                    extra(kind, h, p).wait_send()

    @pl.when(u == 1)
    def _():
        for kind in range(2):
            for p in range(PIECES):
                passed(kind, p).wait_send()

    @pl.when(home)
    def _():
        for kind in range(2):
            whole(kind).wait_send()
            for p in range(PIECES):
                for h in range(2):
                    first(kind, h, p).wait_send()
        for i in range(steps):
            for t in range(3):
                out_copy(i, t).wait_send()

    @pl.when(away)
    def _():
        for p in range(ROW_PARTS):
            row_copy(0, p).wait_send()
            for core in range(CORES):
                row_in(x, core, p).wait_send()
        for i in range(steps):
            cross_copy(i).wait_send()
            for core in range(CORES):
                join_copy(i, core).wait_send()


def fused_block(
    queries, keys, values, sinks, out_weight, up_weight, down_weight, residual, gains, biases
):
    n, m = lax.axis_size("sp"), lax.axis_size("tp")
    depth, hidden = up_weight.shape
    tokens = queries.shape[0]
    own_rows, width = residual.shape
    side_rows, steps = tokens // SIDES, 2 * LAYERS
    vmem, smem = pl.BlockSpec(memory_space=pltpu.VMEM), pl.BlockSpec(memory_space=pltpu.SMEM)
    bf16, dma = jnp.bfloat16, pltpu.SemaphoreType.DMA
    return pl.pallas_call(
        functools.partial(block_kernel, n, m),
        out_shape=jax.ShapeDtypeStruct(residual.shape, bf16),
        in_specs=[vmem] * 3 + [smem] + [vmem] * 2 + [pl.BlockSpec(memory_space=pl.ANY)] * 4,
        out_specs=pl.BlockSpec(memory_space=pltpu.VMEM),
        scratch_shapes=[
            pltpu.VMEM((tokens + WINDOW, keys.shape[1]), bf16),
            pltpu.VMEM((tokens + WINDOW, keys.shape[1]), bf16),
            pltpu.VMEM(out_weight.shape, bf16),
            pltpu.VMEM(residual.shape, bf16),
            pltpu.VMEM(queries.shape, bf16),
            pltpu.VMEM((SIDES, own_rows, queries.shape[1]), bf16),
            pltpu.VMEM(out_weight.shape, bf16),
            pltpu.VMEM((own_rows, width), bf16),
            pltpu.VMEM((own_rows, width), jnp.float32),
            pltpu.VMEM((own_rows, width), bf16),
            pltpu.VMEM((width, hidden), bf16),
            pltpu.VMEM((n, hidden, depth), bf16),
            pltpu.VMEM((own_rows, width), bf16),
            pltpu.VMEM((tokens, width), bf16),
            pltpu.VMEM((tokens, hidden), bf16),
            pltpu.VMEM((steps, tokens, depth), bf16),
            pltpu.VMEM((steps, side_rows, depth), bf16),
            pltpu.VMEM((steps, side_rows, depth), bf16),
            pltpu.VMEM((3, steps, own_rows, depth), bf16),
            pltpu.VMEM((own_rows, width), jnp.float32),
            dma((2,)),
            dma((2,)),
            dma((1,)),
            dma((1,)),
            dma((SIDES,)),
            dma((SIDES,)),
            dma((ROW_PARTS,)),
            dma((ROW_PARTS,)),
            dma((2, 2, PIECES)),
            dma((2, 2, PIECES)),
            dma((2, PIECES)),
            dma((2, LAYERS, PIECES)),
            dma((2, 2, PIECES)),
            dma((2, LAYERS, PIECES)),
            dma((2, LAYERS, PIECES)),
            dma((2,)),
            dma((2,)),
            dma((2, 2, LAYERS, PIECES)),
            dma((2, 2, LAYERS, PIECES)),
            dma((3, ROW_PARTS)),
            dma((m, ROW_PARTS)),
            dma((CORES, ROW_PARTS)),
            dma((steps, 3)),
            dma((steps,)),
            dma((steps,)),
            dma((steps, CORES)),
            dma((3, steps)),
            dma((4,)),
        ],
        compiler_params=pltpu.CompilerParams(
            collective_id=0, has_side_effects=True, vmem_limit_bytes=60 * 1024 * 1024
        ),
    )(
        queries, keys, values, sinks, gains, biases, out_weight, up_weight, down_weight, residual,
    )


def on_device(
    queries, keys, values, residual, sinks, out_weight, up_weight, down_weight, gains, biases
):
    tokens = queries.shape[0]
    rank_tp = lax.axis_index("tp")
    if fits(tokens, up_weight):
        return fused_block(
            queries, keys, values, sinks, out_weight, up_weight, down_weight, residual, gains, biases
        )
    tails = jnp.stack([keys[tokens - WINDOW :], values[tokens - WINDOW :]])
    before = from_behind(tails, "sp", 1)
    offset = lax.axis_index("sp") * tokens
    attended = attend(queries, keys, values, before, sinks, offset, rank_tp)
    part = jnp.dot(attended, out_weight, preferred_element_type=jnp.float32).astype(jnp.bfloat16)
    up_full, down_full = (
        lax.all_gather(up_weight, "sp", axis=0, tiled=True),
        lax.all_gather(down_weight, "sp", axis=1, tiled=True),
    )
    mix = lax.psum_scatter(
        part,
        "tp",
        scatter_dimension=0,
        tiled=True,
    ).astype(jnp.float32)
    normed = layer_norm(deep_alpha * residual.astype(jnp.float32) + mix, gains[0], biases[0])
    whole = lax.all_gather(normed, "tp", axis=0, tiled=True)
    upward = jnp.dot(whole, up_full, preferred_element_type=jnp.float32)
    act = jnp.square(jax.nn.relu(upward)).astype(jnp.bfloat16)
    terms = jnp.dot(act, down_full, preferred_element_type=jnp.float32)
    ffn = lax.psum_scatter(
        terms.astype(jnp.bfloat16), "tp", scatter_dimension=0, tiled=True
    ).astype(jnp.float32)
    return layer_norm(deep_alpha * normed.astype(jnp.float32) + ffn, gains[1], biases[1])


def solution(mesh):
    return jax.shard_map(
        on_device,
        mesh=mesh,
        in_specs=(
            P("sp", "tp"),
            P("sp", "tp"),
            P("sp", "tp"),
            P(("sp", "tp"), None),
            P("tp"),
            P("tp", None),
            P("sp", "tp"),
            P("tp", "sp"),
            P(),
            P(),
        ),
        out_specs=P(("sp", "tp"), None),
        check_vma=False,
    )
```

```python
import functools

import jax
import jax.numpy as jnp
from jax import lax
from jax.experimental import pallas as pl
from jax.experimental.pallas import tpu as pltpu
from jax.sharding import PartitionSpec as P

HEADS = 12
HEAD = 128
WINDOW = 128


deep_alpha = 1.6817928
norm_eps = 1e-05
neg_big = -1e30


def from_behind(block, axis, distance):
    devices = range(lax.axis_size(axis))
    route = [(i - distance, i) for i in devices if i - distance in devices]
    return lax.ppermute(block, axis, route)


def layer_norm(stream, gain, bias):
    mean = jnp.mean(stream, axis=-1, keepdims=True)
    spread = jnp.mean(jnp.square(stream - mean), axis=-1, keepdims=True)
    return ((stream - mean) * lax.rsqrt(spread + norm_eps) * gain + bias).astype(jnp.bfloat16)


def attend(queries, keys, values, before, sinks, offset, rank_tp):
    tokens = keys.shape[0]
    kv_local = keys.shape[1] // HEAD
    heads_local = sinks.shape[0]
    group = heads_local // kv_local
    blocks = tokens // WINDOW
    q_blocks = queries.reshape(blocks, WINDOW, kv_local, group, HEAD)
    key_ext = jnp.concatenate([before[0], keys], axis=0).reshape(tokens + WINDOW, kv_local, HEAD)
    val_ext = jnp.concatenate([before[1], values], axis=0).reshape(tokens + WINDOW, kv_local, HEAD)
    key_win = jnp.concatenate(
        [
            key_ext[:tokens].reshape(blocks, WINDOW, kv_local, HEAD),
            key_ext[WINDOW:].reshape(blocks, WINDOW, kv_local, HEAD),
        ],
        axis=1,
    )
    val_win = jnp.concatenate(
        [
            val_ext[:tokens].reshape(blocks, WINDOW, kv_local, HEAD),
            val_ext[WINDOW:].reshape(blocks, WINDOW, kv_local, HEAD),
        ],
        axis=1,
    )
    logits = jnp.einsum(
        "nqkgd,nskd->nkgqs", q_blocks, key_win, preferred_element_type=jnp.float32
    ) * HEAD ** (-0.5)
    q_index = jnp.arange(WINDOW, dtype=jnp.int32)[:, None]
    k_index = jnp.arange(2 * WINDOW, dtype=jnp.int32)[None, :]
    dist = q_index + WINDOW - k_index
    block_id = jnp.arange(blocks, dtype=jnp.int32)[:, None, None]
    key_pos = offset + block_id * WINDOW - WINDOW + k_index
    valid = (dist >= 0) & (dist < WINDOW) & (key_pos >= 0)
    heads = (jnp.arange(heads_local, dtype=jnp.int32) + rank_tp * heads_local).astype(jnp.float32)
    slopes = jnp.exp2(-8.0 * (heads + 1.0) / HEADS).reshape(kv_local, group)[:, :, None, None]
    logits = logits - slopes * dist.astype(jnp.float32)
    logits = jnp.where(valid[:, None, None], logits, neg_big)
    sink = sinks.reshape(kv_local, group)[:, :, None, None]
    top = jnp.maximum(jnp.max(logits, axis=-1, keepdims=True), sink)
    probs = jnp.exp(logits - top)
    denom = jnp.sum(probs, axis=-1, keepdims=True) + jnp.exp(sink - top)
    weight = (probs / denom).astype(jnp.bfloat16)
    attended = jnp.einsum("nkgqs,nskd->nqkgd", weight, val_win, preferred_element_type=jnp.float32)
    return attended.astype(jnp.bfloat16).reshape(tokens, heads_local * HEAD)


MESH = pl.DeviceIdType.MESH
LANES = 128


def norm_rows(stream, gain, bias):
    mean = jnp.mean(stream, axis=-1, keepdims=True)
    spread = jnp.mean(jnp.square(stream - mean), axis=-1, keepdims=True)
    return (stream - mean) * lax.rsqrt(spread + norm_eps) * gain + bias


ROWS_Y, LAYERS, CORES, SIDES = 2, 4, 2, 2
PIECES = (1, 2)
ROW_PARTS = 2


def fits(tokens, up_weight):
    depth, hidden = up_weight.shape
    return (
        lax.axis_size("sp") == ROWS_Y * LAYERS
        and lax.axis_size("tp") == CORES * SIDES
        and depth % (2 * LANES) == 0
        and hidden % (2 * max(PIECES) * LANES) == 0
        and tokens % (2 * WINDOW) == 0
        and tokens % (SIDES * CORES * ROW_PARTS * 32) == 0
    )


def block_kernel(
    n, m, sinks_ref, gains_ref, biases_ref, q_hbm, k_hbm, v_hbm, proj_hbm, up_ref, down_ref, res_hbm, out_ref,
    q_ref, key_ext, val_ext, proj_ref, res_ref, attended, att_in, proj_in, mix_out, mix_own, mix_in, up_all, down_all,
    normed_own, normed, act, terms, cross_in, joined, terms_in, total,
    tail_send, tail_recv, proj_send, proj_recv, att_send, att_recv, mix_send, mix_recv,
    main_send, extra_send, pass_send, z_recv, first_send, y_send, y_recv, all_send, all_recv,
    d_send, d_recv, row_send, row_recv, fwd_send, out_send, cross_send, cross_recv, join_send, out_recv, local_sem,
):
    me, rank = lax.axis_index("sp"), lax.axis_index("tp")
    depth, hidden = up_ref.shape
    own_rows, width = res_ref.shape
    tokens = q_ref.shape[0]
    q_width = q_ref.shape[1]
    side_rows = tokens // SIDES
    y, z = lax.rem(me, ROWS_Y), lax.div(me, ROWS_Y)
    x, c = lax.div(rank, CORES), lax.rem(rank, CORES)
    half, zl = lax.div(z, 2), lax.rem(z, 2)
    oy, ox, oc = 1 - y, 1 - x, 1 - c
    oz = z + 1 - 2 * zl
    u = zl + half - 2 * zl * half
    step_rows = 32

    home = c == zl
    away = c != zl
    h1 = 1 - lax.rem(c + zl, 2)

    def layer(w):
        return w + half * (LAYERS - 1 - 2 * w)

    def source(k):
        return layer(u if k == 0 else 1 - u if k == 1 else k)

    def at(x_, y_, z_, c_):
        return (z_ * ROWS_Y + y_, x_ * CORES + c_)

    barrier = pltpu.get_barrier_semaphore()
    partners = [at(x, y, z, oc)]
    for k in range(1, LAYERS):
        for core in range(CORES):
            partners.append(at(x, y, lax.rem(z + k, LAYERS), core))
    for core in range(CORES):
        partners.append(at(x, oy, z, core))
        partners.append(at(ox, y, z, core))
    partners.append(at(x, oy, lax.rem(z + 2 * y - 1 + LAYERS, LAYERS), c))
    for there in partners:
        pl.semaphore_signal(barrier, inc=1, device_id=there, device_id_type=MESH)
    loads = [
        pltpu.make_async_copy(k_hbm, key_ext.at[pl.ds(WINDOW, tokens)], local_sem.at[4]),
        pltpu.make_async_copy(v_hbm, val_ext.at[pl.ds(WINDOW, tokens)], local_sem.at[5]),
        pltpu.make_async_copy(q_hbm, q_ref, local_sem.at[6]),
    ]
    for copy in loads:
        copy.start()
    pl.semaphore_wait(barrier, len(partners))

    def remote(source, target, send, recv, device):
        return pltpu.make_async_remote_copy(
            src_ref=source, dst_ref=target, send_sem=send, recv_sem=recv,
            device_id=device, device_id_type=MESH,
        )

    def held(kind, s, h, p):
        if kind == 0:
            rows = depth // (2 * PIECES[kind])
            off = s * depth + h * (depth // 2) + p * rows
            return up_all.at[pl.ds(pl.multiple_of(off, rows), rows)]
        rows = hidden // (2 * PIECES[kind])
        off = h * (hidden // 2) + p * rows
        return down_all.at[s, pl.ds(pl.multiple_of(off, rows), rows)]

    def own_piece(kind, h, p):
        ref = up_ref if kind == 0 else down_ref
        rows = ref.shape[0] // (2 * PIECES[kind])
        return ref.at[pl.ds(h * (ref.shape[0] // 2) + p * rows, rows)]

    w_main = h1 * (u + 2) + (1 - h1) * (u + 1)
    k_main = h1 * (3 - u) + (1 - h1) * (1 + u)

    def main(kind, h, p):
        return remote(
            own_piece(kind, h, p), held(kind, me, h, p), main_send.at[kind, h, p],
            z_recv.at[kind, k_main, p], at(x, y, layer(w_main), h),
        )

    def extra(kind, h, p):
        return remote(
            own_piece(kind, h, p), held(kind, me, h, p), extra_send.at[kind, h, p],
            z_recv.at[kind, 1, p], at(x, y, layer(0), h),
        )

    extra_here = (u == 1) & away

    def column(k, other):
        return source(k) * ROWS_Y + (oy if other else y)

    def z_piece(kind, k, p):
        ref = held(kind, column(k, 0), c, p)
        return remote(ref, ref, pass_send.at[kind, p], z_recv.at[kind, k, p], at(x, y, z, oc))

    def passed(kind, p):
        ref = held(kind, column(1, 0), c, p)
        return remote(
            ref, ref, pass_send.at[kind, p], z_recv.at[kind, 3, p], at(x, y, layer(3), c)
        )

    def first(kind, h, p):
        return remote(
            own_piece(kind, h, p), held(kind, me, h, p), first_send.at[kind, h, p],
            y_recv.at[kind, 0, p], at(x, oy, z, h),
        )

    def y_out(kind, k, p):
        ref = held(kind, column(k, 0), c, p)
        return remote(
            ref, ref, y_send.at[kind, k, p], y_recv.at[kind, k, p], at(x, oy, z, c)
        )

    def y_in(kind, k, p):
        ref = held(kind, column(k, 1), c, p)
        return remote(
            ref, ref, y_send.at[kind, k, p], y_recv.at[kind, k, p], at(x, oy, z, c)
        )

    def across(kind, other, k, p, h):
        ref = held(kind, column(k, other), h, p)
        return remote(
            ref, ref, d_send.at[kind, other, k, p], d_recv.at[kind, other, k, p],
            at(x, y, z, oc),
        )

    def whole(kind):
        ref = up_ref if kind == 0 else down_ref
        if kind == 0:
            target = up_all.at[pl.ds(pl.multiple_of(me * depth, depth), depth)]
        else:
            target = down_all.at[me]
        return remote(ref, target, all_send.at[kind], all_recv.at[kind], at(x, y, z, oc))

    def launch_local(kind):
        @pl.when(home)
        def _():
            whole(kind).start()
            for p in range(PIECES[kind]):
                for h in range(2):
                    first(kind, h, p).start()

    def launch_main(kind):
        for p in range(PIECES[kind]):
            for h in range(2):
                main(kind, h, p).start()

    def launch_extra(kind):
        @pl.when(extra_here)
        def _():
            for p in range(PIECES[kind]):
                for h in range(2):
                    extra(kind, h, p).start()

    def serve_z(kind, k):
        for p in range(PIECES[kind]):
            z_piece(kind, k, p).wait_recv()
            if k == 1 and kind == 0:
                @pl.when(u == 1)
                def _():
                    passed(kind, p).start()
            y_out(kind, k, p).start()
            across(kind, 0, k, p, c).start()

    def serve_y(kind, k):
        for p in range(PIECES[kind]):
            y_in(kind, k, p).wait_recv()
            across(kind, 1, k, p, c).start()

    def need(kind, other, k):
        if k == 0 and not other:
            @pl.when(away)
            def _():
                whole(kind).wait_recv()

            @pl.when(home)
            def _():
                own_block(kind).wait()
            return
        for p in range(PIECES[kind]):
            across(kind, other, k, p, oc).wait_recv()

    after = lax.rem(me + 1, n)
    tails = [
        remote(
            ref.at[pl.ds(tokens - WINDOW, WINDOW)], ext.at[pl.ds(0, WINDOW)],
            tail_send.at[i], tail_recv.at[i], (after, rank),
        )
        for i, (ref, ext) in enumerate(((k_hbm, key_ext), (v_hbm, val_ext)))
    ]
    for copy in tails:
        copy.start()
    launch_main(0)
    launch_extra(0)
    proj_copy = remote(proj_hbm, proj_in, proj_send.at[0], proj_recv.at[0], at(x, y, z, oc))
    proj_copy.start()
    launch_local(0)
    proj_local = pltpu.make_async_copy(proj_hbm, proj_ref, local_sem.at[0])
    res_local = pltpu.make_async_copy(res_hbm, res_ref, local_sem.at[1])
    proj_local.start()
    res_local.start()

    def own_block(kind):
        if kind == 0:
            target = up_all.at[pl.ds(pl.multiple_of(me * depth, depth), depth)]
            return pltpu.make_async_copy(up_ref, target, local_sem.at[2])
        return pltpu.make_async_copy(down_ref, down_all.at[me], local_sem.at[3])

    @pl.when(home)
    def _():
        own_block(0).start()
        own_block(1).start()


    blocks = tokens // WINDOW
    heads_local = q_width // HEAD
    group = heads_local // (k_hbm.shape[1] // HEAD)

    slopes = [
        jnp.exp2(
            jnp.full((1, 2 * WINDOW), -8.0 / HEADS, jnp.float32)
            * (rank * heads_local + (h + 1)).astype(jnp.float32)
        )
        for h in range(heads_local)
    ]

    def windows(first_block, count):
        @pl.loop(0, count)
        def _(i):
            start = pl.multiple_of((first_block + i) * WINDOW, WINDOW)
            rows, span = pl.ds(start, WINDOW), pl.ds(start, 2 * WINDOW)
            q_index = lax.broadcasted_iota(jnp.int32, (WINDOW, 2 * WINDOW), 0)
            k_index = lax.broadcasted_iota(jnp.int32, (WINDOW, 2 * WINDOW), 1)
            dist = q_index + WINDOW - k_index
            key_pos = me * tokens + start - WINDOW + k_index
            valid = (dist >= 0) & (dist < WINDOW) & (key_pos >= 0)
            far = dist.astype(jnp.float32)
            for h in range(heads_local):
                columns = slice(h * HEAD, (h + 1) * HEAD)
                shared = slice(h // group * HEAD, (h // group + 1) * HEAD)
                logits = lax.dot_general(
                    q_ref[rows, columns], key_ext[span, shared], (((1,), (1,)), ((), ())),
                    preferred_element_type=jnp.float32,
                ) * HEAD ** (-0.5)
                logits = jnp.where(valid, logits - slopes[h] * far, neg_big)
                sink = sinks_ref[h]
                top = jnp.maximum(jnp.max(logits, axis=-1, keepdims=True), sink)
                probs = jnp.exp(logits - top)
                denom = jnp.sum(probs, axis=-1, keepdims=True) + jnp.exp(sink - top)
                weight = (probs / denom).astype(jnp.bfloat16)
                attended[rows, columns] = jnp.dot(
                    weight, val_ext[span, shared], preferred_element_type=jnp.float32
                ).astype(jnp.bfloat16)

    def rows_of(side, core):
        start = side * side_rows + core * own_rows
        return pl.ds(pl.multiple_of(start, own_rows), own_rows)

    def swap(i, side):
        return remote(
            attended.at[rows_of(side, oc)], att_in.at[i], att_send.at[i], att_recv.at[i],
            at(x, y, z, oc),
        )

    tile = 2 * LANES

    def project(i, side, target):
        @pl.loop(0, width // tile)
        def _(j):
            columns = pl.ds(pl.multiple_of(j * tile, tile), tile)
            target[:, columns] = (
                jnp.dot(
                    attended[rows_of(side, c)], proj_ref[:, columns],
                    preferred_element_type=jnp.float32,
                )
                + jnp.dot(att_in[i], proj_in[:, columns], preferred_element_type=jnp.float32)
            ).astype(target.dtype)

    part_rows = own_rows // ROW_PARTS

    def mix_copy(p):
        rows = pl.ds(p * part_rows, part_rows)
        return remote(
            mix_out.at[rows], mix_in.at[rows], mix_send.at[p], mix_recv.at[p], at(ox, y, z, c)
        )

    for copy in loads:
        copy.wait()
    windows(ox * (blocks // 2) + 1, blocks // 2 - 1)
    for copy in tails:
        copy.wait_recv()
    windows(ox * (blocks // 2), 1)
    swap(0, ox).start()
    proj_local.wait()
    proj_copy.wait_recv()
    swap(0, ox).wait_recv()
    project(0, ox, mix_out)
    for p in range(ROW_PARTS):
        mix_copy(p).start()
    windows(x * (blocks // 2), blocks // 2)
    swap(1, x).start()
    serve_z(0, 1)
    swap(1, x).wait_recv()
    project(1, x, mix_own)
    res_local.wait()

    def rank_rows(r, p):
        start = r * own_rows + p * part_rows
        return pl.ds(pl.multiple_of(start, part_rows), part_rows)

    def row_copy(t, p):
        source_ref, rows = normed_own.at[pl.ds(p * part_rows, part_rows)], rank_rows(rank, p)
        there = [at(x, y, z, oc), at(ox, y, z, zl), at(x, y, oz, zl)][t]
        return remote(
            source_ref, normed.at[rows], row_send.at[t, p], row_recv.at[rank, p], there
        )

    def row_in(side, core, p):
        r = side * CORES + core
        ref = normed.at[rank_rows(r, p)]
        return remote(ref, ref, fwd_send.at[core, p], row_recv.at[r, p], at(ox, y, z, c))

    for p in range(ROW_PARTS):
        mix_copy(p).wait_recv()

        @pl.loop(0, part_rows // step_rows)
        def _(i):
            start = pl.multiple_of(p * part_rows + i * step_rows, step_rows)
            rows = pl.ds(start, step_rows)
            mix = mix_own[rows] + mix_in[rows].astype(jnp.float32)
            stream = deep_alpha * res_ref[rows].astype(jnp.float32) + mix
            made = norm_rows(stream, gains_ref[0:1], biases_ref[0:1]).astype(jnp.bfloat16)
            normed_own[rows] = made

            @pl.when(home)
            def _():
                mine = pl.ds(pl.multiple_of(rank * own_rows + start, step_rows), step_rows)
                normed[mine] = made

        row_copy(2, p).start()
        row_copy(1, p).start()

        @pl.when(away)
        def _():
            row_copy(0, p).start()

    serve_z(0, 2)

    @pl.when(u == 0)
    def _():
        launch_local(1)

    @pl.when((u == 0) & away)
    def _():
        launch_main(1)

    serve_y(0, 0)
    serve_y(0, 1)

    serve_z(0, 3)

    @pl.when(((u == 1) & away) | ((u == 0) & home))
    def _():
        launch_main(1)

    @pl.when(u == 1)
    def _():
        launch_local(1)

    @pl.when(away)
    def _():
        for p in range(ROW_PARTS):
            for core in range(CORES):
                row_in(x, core, p).wait_recv()
                row_in(x, core, p).start()

    launch_extra(1)
    serve_y(0, 2)
    serve_y(0, 3)
    for k in range(LAYERS):
        for other in range(2):
            need(0, other, k)

    for p in range(ROW_PARTS):
        for core in range(CORES):
            row_in(ox, core, p).wait_recv()

        @pl.when(home)
        def _():
            row_in(x, oc, p).wait_recv()

    tiles = hidden // tile

    def upward(first, last):
        @pl.loop(first, last)
        def _(i):
            columns = pl.ds(pl.multiple_of(i * tile, tile), tile)
            made = jnp.dot(normed[...], up_all[:, columns], preferred_element_type=jnp.float32)
            act[:, columns] = jnp.square(jnp.maximum(made, 0.0)).astype(jnp.bfloat16)

    parts = 4
    for part in range(parts):
        upward(part * tiles // parts, (part + 1) * tiles // parts)
        if part == 0:
            @pl.when((u == 1) & home)
            def _():
                launch_main(1)

            serve_z(1, 1)

    @pl.when(u == 1)
    def _():
        for p in range(PIECES[1]):
            passed(1, p).start()

    steps = 2 * LAYERS

    def out_copy(i, t):
        r = [x * CORES + oc, ox * CORES, ox * CORES + 1][t]
        rows = pl.ds(pl.multiple_of(r * own_rows, own_rows), own_rows)
        there = [at(x, y, z, oc), at(ox, y, z, 0), at(ox, y, z, 1)][t]
        slot = 0 if t == 0 else 1
        return remote(
            terms.at[i, rows], terms_in.at[slot, i], out_send.at[i, t], out_recv.at[slot, i], there
        )

    def cross_copy(i):
        rows = pl.ds(pl.multiple_of(ox * side_rows, side_rows), side_rows)
        return remote(
            terms.at[i, rows], cross_in.at[i], cross_send.at[i], cross_recv.at[i], at(ox, y, z, c)
        )

    def join_copy(i, core):
        return remote(
            joined.at[i, pl.ds(core * own_rows, own_rows)], terms_in.at[2, i],
            join_send.at[i, core], out_recv.at[2, i], at(x, y, oz, core),
        )

    held_rows = pl.ds(pl.multiple_of(rank * own_rows, own_rows), own_rows)

    def downward(i):
        s = column(i // 2, i % 2)
        terms[i] = jnp.dot(
            act[...], down_all[s], preferred_element_type=jnp.float32
        ).astype(jnp.bfloat16)

        @pl.when(home)
        def _():
            for t in range(3):
                out_copy(i, t).start()
            terms_in[0, i] = terms[i, held_rows]

        @pl.when(away)
        def _():
            cross_copy(i).start()

    def join(i):
        @pl.when(away)
        def _():
            cross_copy(i).wait_recv()
            rows = pl.ds(pl.multiple_of(x * side_rows, side_rows), side_rows)
            joined[i] = (
                terms[i, rows].astype(jnp.float32) + cross_in[i].astype(jnp.float32)
            ).astype(jnp.bfloat16)
            for core in range(CORES):
                join_copy(i, core).start()

    def collect(k):
        for other in range(2):
            i = 2 * k + other
            i2 = 2 * (1 - k if k < 2 else k) + other

            @pl.when(away)
            def _():
                out_copy(i, 0).wait_recv()

            out_copy(i, 1).wait_recv()
            join_copy(i2, 0).wait_recv()
            columns = pl.ds(pl.multiple_of(column(k, other) * depth, depth), depth)
            block = terms_in[0, i].astype(jnp.float32)
            block += terms_in[1, i].astype(jnp.float32)
            block += terms_in[2, i2].astype(jnp.float32)
            total[:, columns] = deep_alpha * normed_own[:, columns].astype(jnp.float32) + block

    before = {
        1: [(serve_y, 0)],
        2: [(serve_z, 2)],
        3: [(serve_y, 1)],
        4: [(serve_z, 3)],
        5: [(serve_y, 2)],
        7: [(serve_y, 3)],
    }
    for i in range(steps):
        k, other = i // 2, i % 2
        for serve, at_k in before.get(i, []):
            serve(1, at_k)
        need(1, other, k)
        downward(i)
        if i == 6:
            for j in range(i):
                join(j)
        if i > 6:
            join(i - 1)
    join(steps - 1)
    for k in range(LAYERS):
        collect(k)

    @pl.loop(0, own_rows // step_rows)
    def _(i):
        rows = pl.ds(pl.multiple_of(i * step_rows, step_rows), step_rows)
        out_ref[rows] = norm_rows(total[rows], gains_ref[1:2], biases_ref[1:2]).astype(jnp.bfloat16)

    for copy in tails:
        copy.wait_send()
    proj_copy.wait_send()
    swap(0, ox).wait_send()
    swap(1, x).wait_send()
    for p in range(ROW_PARTS):
        mix_copy(p).wait_send()
        row_copy(1, p).wait_send()
        row_copy(2, p).wait_send()
    for kind in range(2):
        for p in range(PIECES[kind]):
            for h in range(2):
                main(kind, h, p).wait_send()
            for k in range(LAYERS):
                if k > 0:
                    y_out(kind, k, p).wait_send()
                    across(kind, 0, k, p, c).wait_send()
                across(kind, 1, k, p, c).wait_send()

    @pl.when(extra_here)
    def _():
        for kind in range(2):
            for p in range(PIECES[kind]):
                for h in range(2):
                    extra(kind, h, p).wait_send()

    @pl.when(u == 1)
    def _():
        for kind in range(2):
            for p in range(PIECES[kind]):
                passed(kind, p).wait_send()

    @pl.when(home)
    def _():
        for kind in range(2):
            whole(kind).wait_send()
            for p in range(PIECES[kind]):
                for h in range(2):
                    first(kind, h, p).wait_send()
        for i in range(steps):
            for t in range(3):
                out_copy(i, t).wait_send()

    @pl.when(away)
    def _():
        for p in range(ROW_PARTS):
            row_copy(0, p).wait_send()
            for core in range(CORES):
                row_in(x, core, p).wait_send()
        for i in range(steps):
            cross_copy(i).wait_send()
            for core in range(CORES):
                join_copy(i, core).wait_send()


def fused_block(
    queries, keys, values, sinks, out_weight, up_weight, down_weight, residual, gains, biases
):
    n, m = lax.axis_size("sp"), lax.axis_size("tp")
    depth, hidden = up_weight.shape
    tokens = queries.shape[0]
    own_rows, width = residual.shape
    side_rows, steps = tokens // SIDES, 2 * LAYERS
    vmem, smem = pl.BlockSpec(memory_space=pltpu.VMEM), pl.BlockSpec(memory_space=pltpu.SMEM)
    bf16, dma = jnp.bfloat16, pltpu.SemaphoreType.DMA
    return pl.pallas_call(
        functools.partial(block_kernel, n, m),
        out_shape=jax.ShapeDtypeStruct(residual.shape, bf16),
        in_specs=[smem] + [vmem] * 2 + [pl.BlockSpec(memory_space=pl.ANY)] * 7,
        out_specs=pl.BlockSpec(memory_space=pltpu.VMEM),
        scratch_shapes=[
            pltpu.VMEM(queries.shape, bf16),
            pltpu.VMEM((tokens + WINDOW, keys.shape[1]), bf16),
            pltpu.VMEM((tokens + WINDOW, keys.shape[1]), bf16),
            pltpu.VMEM(out_weight.shape, bf16),
            pltpu.VMEM(residual.shape, bf16),
            pltpu.VMEM(queries.shape, bf16),
            pltpu.VMEM((SIDES, own_rows, queries.shape[1]), bf16),
            pltpu.VMEM(out_weight.shape, bf16),
            pltpu.VMEM((own_rows, width), bf16),
            pltpu.VMEM((own_rows, width), jnp.float32),
            pltpu.VMEM((own_rows, width), bf16),
            pltpu.VMEM((width, hidden), bf16),
            pltpu.VMEM((n, hidden, depth), bf16),
            pltpu.VMEM((own_rows, width), bf16),
            pltpu.VMEM((tokens, width), bf16),
            pltpu.VMEM((tokens, hidden), bf16),
            pltpu.VMEM((steps, tokens, depth), bf16),
            pltpu.VMEM((steps, side_rows, depth), bf16),
            pltpu.VMEM((steps, side_rows, depth), bf16),
            pltpu.VMEM((3, steps, own_rows, depth), bf16),
            pltpu.VMEM((own_rows, width), jnp.float32),
            dma((2,)),
            dma((2,)),
            dma((1,)),
            dma((1,)),
            dma((SIDES,)),
            dma((SIDES,)),
            dma((ROW_PARTS,)),
            dma((ROW_PARTS,)),
            dma((2, 2, max(PIECES))),
            dma((2, 2, max(PIECES))),
            dma((2, max(PIECES))),
            dma((2, LAYERS, max(PIECES))),
            dma((2, 2, max(PIECES))),
            dma((2, LAYERS, max(PIECES))),
            dma((2, LAYERS, max(PIECES))),
            dma((2,)),
            dma((2,)),
            dma((2, 2, LAYERS, max(PIECES))),
            dma((2, 2, LAYERS, max(PIECES))),
            dma((3, ROW_PARTS)),
            dma((m, ROW_PARTS)),
            dma((CORES, ROW_PARTS)),
            dma((steps, 3)),
            dma((steps,)),
            dma((steps,)),
            dma((steps, CORES)),
            dma((3, steps)),
            dma((7,)),
        ],
        compiler_params=pltpu.CompilerParams(
            collective_id=0, has_side_effects=True, vmem_limit_bytes=60 * 1024 * 1024
        ),
    )(
        sinks, gains, biases, queries, keys, values, out_weight, up_weight, down_weight, residual,
    )


def on_device(
    queries, keys, values, residual, sinks, out_weight, up_weight, down_weight, gains, biases
):
    tokens = queries.shape[0]
    rank_tp = lax.axis_index("tp")
    if fits(tokens, up_weight):
        return fused_block(
            queries, keys, values, sinks, out_weight, up_weight, down_weight, residual, gains, biases
        )
    tails = jnp.stack([keys[tokens - WINDOW :], values[tokens - WINDOW :]])
    before = from_behind(tails, "sp", 1)
    offset = lax.axis_index("sp") * tokens
    attended = attend(queries, keys, values, before, sinks, offset, rank_tp)
    part = jnp.dot(attended, out_weight, preferred_element_type=jnp.float32).astype(jnp.bfloat16)
    up_full, down_full = (
        lax.all_gather(up_weight, "sp", axis=0, tiled=True),
        lax.all_gather(down_weight, "sp", axis=1, tiled=True),
    )
    mix = lax.psum_scatter(
        part,
        "tp",
        scatter_dimension=0,
        tiled=True,
    ).astype(jnp.float32)
    normed = layer_norm(deep_alpha * residual.astype(jnp.float32) + mix, gains[0], biases[0])
    whole = lax.all_gather(normed, "tp", axis=0, tiled=True)
    upward = jnp.dot(whole, up_full, preferred_element_type=jnp.float32)
    act = jnp.square(jax.nn.relu(upward)).astype(jnp.bfloat16)
    terms = jnp.dot(act, down_full, preferred_element_type=jnp.float32)
    ffn = lax.psum_scatter(
        terms.astype(jnp.bfloat16), "tp", scatter_dimension=0, tiled=True
    ).astype(jnp.float32)
    return layer_norm(deep_alpha * normed.astype(jnp.float32) + ffn, gains[1], biases[1])


def solution(mesh):
    return jax.shard_map(
        on_device,
        mesh=mesh,
        in_specs=(
            P("sp", "tp"),
            P("sp", "tp"),
            P("sp", "tp"),
            P(("sp", "tp"), None),
            P("tp"),
            P("tp", None),
            P("sp", "tp"),
            P("tp", "sp"),
            P(),
            P(),
        ),
        out_specs=P(("sp", "tp"), None),
        check_vma=False,
    )
```

```python
import functools

import jax
import jax.numpy as jnp
from jax import lax
from jax.experimental import pallas as pl
from jax.experimental.pallas import tpu as pltpu
from jax.sharding import PartitionSpec as P

HEADS = 12
HEAD = 128
WINDOW = 128


deep_alpha = 1.6817928
norm_eps = 1e-05
neg_big = -1e30


def from_behind(block, axis, distance):
    devices = range(lax.axis_size(axis))
    route = [(i - distance, i) for i in devices if i - distance in devices]
    return lax.ppermute(block, axis, route)


def layer_norm(stream, gain, bias):
    mean = jnp.mean(stream, axis=-1, keepdims=True)
    spread = jnp.mean(jnp.square(stream - mean), axis=-1, keepdims=True)
    return ((stream - mean) * lax.rsqrt(spread + norm_eps) * gain + bias).astype(jnp.bfloat16)


def attend(queries, keys, values, before, sinks, offset, rank_tp):
    tokens = keys.shape[0]
    kv_local = keys.shape[1] // HEAD
    heads_local = sinks.shape[0]
    group = heads_local // kv_local
    blocks = tokens // WINDOW
    q_blocks = queries.reshape(blocks, WINDOW, kv_local, group, HEAD)
    key_ext = jnp.concatenate([before[0], keys], axis=0).reshape(tokens + WINDOW, kv_local, HEAD)
    val_ext = jnp.concatenate([before[1], values], axis=0).reshape(tokens + WINDOW, kv_local, HEAD)
    key_win = jnp.concatenate(
        [
            key_ext[:tokens].reshape(blocks, WINDOW, kv_local, HEAD),
            key_ext[WINDOW:].reshape(blocks, WINDOW, kv_local, HEAD),
        ],
        axis=1,
    )
    val_win = jnp.concatenate(
        [
            val_ext[:tokens].reshape(blocks, WINDOW, kv_local, HEAD),
            val_ext[WINDOW:].reshape(blocks, WINDOW, kv_local, HEAD),
        ],
        axis=1,
    )
    logits = jnp.einsum(
        "nqkgd,nskd->nkgqs", q_blocks, key_win, preferred_element_type=jnp.float32
    ) * HEAD ** (-0.5)
    q_index = jnp.arange(WINDOW, dtype=jnp.int32)[:, None]
    k_index = jnp.arange(2 * WINDOW, dtype=jnp.int32)[None, :]
    dist = q_index + WINDOW - k_index
    block_id = jnp.arange(blocks, dtype=jnp.int32)[:, None, None]
    key_pos = offset + block_id * WINDOW - WINDOW + k_index
    valid = (dist >= 0) & (dist < WINDOW) & (key_pos >= 0)
    heads = (jnp.arange(heads_local, dtype=jnp.int32) + rank_tp * heads_local).astype(jnp.float32)
    slopes = jnp.exp2(-8.0 * (heads + 1.0) / HEADS).reshape(kv_local, group)[:, :, None, None]
    logits = logits - slopes * dist.astype(jnp.float32)
    logits = jnp.where(valid[:, None, None], logits, neg_big)
    sink = sinks.reshape(kv_local, group)[:, :, None, None]
    top = jnp.maximum(jnp.max(logits, axis=-1, keepdims=True), sink)
    probs = jnp.exp(logits - top)
    denom = jnp.sum(probs, axis=-1, keepdims=True) + jnp.exp(sink - top)
    weight = (probs / denom).astype(jnp.bfloat16)
    attended = jnp.einsum("nkgqs,nskd->nqkgd", weight, val_win, preferred_element_type=jnp.float32)
    return attended.astype(jnp.bfloat16).reshape(tokens, heads_local * HEAD)


MESH = pl.DeviceIdType.MESH
LANES = 128


def norm_rows(stream, gain, bias):
    mean = jnp.mean(stream, axis=-1, keepdims=True)
    spread = jnp.mean(jnp.square(stream - mean), axis=-1, keepdims=True)
    return (stream - mean) * lax.rsqrt(spread + norm_eps) * gain + bias


ROWS_Y, LAYERS, CORES, SIDES = 2, 4, 2, 2
PIECES = (1, 2)
ROW_PARTS = 2


def fits(tokens, up_weight):
    depth, hidden = up_weight.shape
    return (
        lax.axis_size("sp") == ROWS_Y * LAYERS
        and lax.axis_size("tp") == CORES * SIDES
        and depth % (2 * LANES) == 0
        and hidden % (2 * max(PIECES) * LANES) == 0
        and tokens % (2 * WINDOW) == 0
        and tokens % (SIDES * CORES * ROW_PARTS * 32) == 0
    )


def block_kernel(
    n, m, sinks_ref, gains_ref, biases_ref, q_hbm, k_hbm, v_hbm, proj_hbm, up_ref, down_ref, res_hbm, out_ref,
    q_ref, key_ext, val_ext, proj_ref, res_ref, attended, att_in, proj_in, mix_out, mix_own, mix_in, up_all, down_all,
    normed_own, normed, act, terms, cross_in, joined, terms_in, total,
    tail_send, tail_recv, proj_send, proj_recv, att_send, att_recv, mix_send, mix_recv,
    main_send, extra_send, pass_send, z_recv, first_send, y_send, y_recv, all_send, all_recv,
    d_send, d_recv, row_send, row_recv, fwd_send, out_send, cross_send, cross_recv, join_send, out_recv, local_sem,
):
    me, rank = lax.axis_index("sp"), lax.axis_index("tp")
    depth, hidden = up_ref.shape
    own_rows, width = res_ref.shape
    tokens = q_ref.shape[0]
    q_width = q_ref.shape[1]
    side_rows = tokens // SIDES
    y, z = lax.rem(me, ROWS_Y), lax.div(me, ROWS_Y)
    x, c = lax.div(rank, CORES), lax.rem(rank, CORES)
    half, zl = lax.div(z, 2), lax.rem(z, 2)
    oy, ox, oc = 1 - y, 1 - x, 1 - c
    oz = z + 1 - 2 * zl
    u = zl + half - 2 * zl * half
    step_rows = 32

    home = c == zl
    away = c != zl
    h1 = 1 - lax.rem(c + zl, 2)

    def layer(w):
        return w + half * (LAYERS - 1 - 2 * w)

    def source(k):
        return layer(u if k == 0 else 1 - u if k == 1 else k)

    def at(x_, y_, z_, c_):
        return (z_ * ROWS_Y + y_, x_ * CORES + c_)

    barrier = pltpu.get_barrier_semaphore()
    partners = [at(x, y, z, oc)]
    for k in range(1, LAYERS):
        for core in range(CORES):
            partners.append(at(x, y, lax.rem(z + k, LAYERS), core))
    for core in range(CORES):
        partners.append(at(x, oy, z, core))
        partners.append(at(ox, y, z, core))
    partners.append(at(x, oy, lax.rem(z + 2 * y - 1 + LAYERS, LAYERS), c))
    for there in partners:
        pl.semaphore_signal(barrier, inc=1, device_id=there, device_id_type=MESH)
    loads = [
        pltpu.make_async_copy(k_hbm, key_ext.at[pl.ds(WINDOW, tokens)], local_sem.at[4]),
        pltpu.make_async_copy(v_hbm, val_ext.at[pl.ds(WINDOW, tokens)], local_sem.at[5]),
        pltpu.make_async_copy(q_hbm, q_ref, local_sem.at[6]),
    ]
    for copy in loads:
        copy.start()
    pl.semaphore_wait(barrier, len(partners))

    def remote(source, target, send, recv, device):
        return pltpu.make_async_remote_copy(
            src_ref=source, dst_ref=target, send_sem=send, recv_sem=recv,
            device_id=device, device_id_type=MESH,
        )

    def held(kind, s, h, p):
        if kind == 0:
            rows = depth // (2 * PIECES[kind])
            off = s * depth + h * (depth // 2) + p * rows
            return up_all.at[pl.ds(pl.multiple_of(off, rows), rows)]
        rows = hidden // (2 * PIECES[kind])
        off = h * (hidden // 2) + p * rows
        return down_all.at[s, pl.ds(pl.multiple_of(off, rows), rows)]

    def own_piece(kind, h, p):
        ref = up_ref if kind == 0 else down_ref
        rows = ref.shape[0] // (2 * PIECES[kind])
        return ref.at[pl.ds(h * (ref.shape[0] // 2) + p * rows, rows)]

    w_main = h1 * (u + 2) + (1 - h1) * (u + 1)
    k_main = h1 * (3 - u) + (1 - h1) * (1 + u)

    def main(kind, h, p):
        return remote(
            own_piece(kind, h, p), held(kind, me, h, p), main_send.at[kind, h, p],
            z_recv.at[kind, k_main, p], at(x, y, layer(w_main), h),
        )

    def extra(kind, h, p):
        return remote(
            own_piece(kind, h, p), held(kind, me, h, p), extra_send.at[kind, h, p],
            z_recv.at[kind, 1, p], at(x, y, layer(0), h),
        )

    extra_here = (u == 1) & away

    def column(k, other):
        return source(k) * ROWS_Y + (oy if other else y)

    def z_piece(kind, k, p):
        ref = held(kind, column(k, 0), c, p)
        return remote(ref, ref, pass_send.at[kind, p], z_recv.at[kind, k, p], at(x, y, z, oc))

    def passed(kind, p):
        ref = held(kind, column(1, 0), c, p)
        return remote(
            ref, ref, pass_send.at[kind, p], z_recv.at[kind, 3, p], at(x, y, layer(3), c)
        )

    def first(kind, h, p):
        return remote(
            own_piece(kind, h, p), held(kind, me, h, p), first_send.at[kind, h, p],
            y_recv.at[kind, 0, p], at(x, oy, z, h),
        )

    def y_out(kind, k, p):
        ref = held(kind, column(k, 0), c, p)
        return remote(
            ref, ref, y_send.at[kind, k, p], y_recv.at[kind, k, p], at(x, oy, z, c)
        )

    def y_in(kind, k, p):
        ref = held(kind, column(k, 1), c, p)
        return remote(
            ref, ref, y_send.at[kind, k, p], y_recv.at[kind, k, p], at(x, oy, z, c)
        )

    def across(kind, other, k, p, h):
        ref = held(kind, column(k, other), h, p)
        return remote(
            ref, ref, d_send.at[kind, other, k, p], d_recv.at[kind, other, k, p],
            at(x, y, z, oc),
        )

    def whole(kind):
        ref = up_ref if kind == 0 else down_ref
        if kind == 0:
            target = up_all.at[pl.ds(pl.multiple_of(me * depth, depth), depth)]
        else:
            target = down_all.at[me]
        return remote(ref, target, all_send.at[kind], all_recv.at[kind], at(x, y, z, oc))

    def launch_local(kind):
        @pl.when(home)
        def _():
            whole(kind).start()
            for p in range(PIECES[kind]):
                for h in range(2):
                    first(kind, h, p).start()

    def launch_main(kind):
        for p in range(PIECES[kind]):
            for h in range(2):
                main(kind, h, p).start()

    def launch_extra(kind):
        @pl.when(extra_here)
        def _():
            for p in range(PIECES[kind]):
                for h in range(2):
                    extra(kind, h, p).start()

    def serve_z(kind, k):
        for p in range(PIECES[kind]):
            z_piece(kind, k, p).wait_recv()
            if k == 1 and kind == 0:
                @pl.when(u == 1)
                def _():
                    passed(kind, p).start()
            y_out(kind, k, p).start()
            across(kind, 0, k, p, c).start()

    def serve_y(kind, k):
        for p in range(PIECES[kind]):
            y_in(kind, k, p).wait_recv()
            across(kind, 1, k, p, c).start()

    def need(kind, other, k):
        if k == 0 and not other:
            @pl.when(away)
            def _():
                whole(kind).wait_recv()

            @pl.when(home)
            def _():
                own_block(kind).wait()
            return
        for p in range(PIECES[kind]):
            across(kind, other, k, p, oc).wait_recv()

    after = lax.rem(me + 1, n)
    tails = [
        remote(
            ref.at[pl.ds(tokens - WINDOW, WINDOW)], ext.at[pl.ds(0, WINDOW)],
            tail_send.at[i], tail_recv.at[i], (after, rank),
        )
        for i, (ref, ext) in enumerate(((k_hbm, key_ext), (v_hbm, val_ext)))
    ]
    @pl.when(me != n - 1)
    def _():
        for copy in tails:
            copy.start()

    launch_main(0)
    launch_extra(0)
    proj_copy = remote(proj_hbm, proj_in, proj_send.at[0], proj_recv.at[0], at(x, y, z, oc))
    proj_copy.start()
    launch_local(0)
    proj_local = pltpu.make_async_copy(proj_hbm, proj_ref, local_sem.at[0])
    res_local = pltpu.make_async_copy(res_hbm, res_ref, local_sem.at[1])
    proj_local.start()
    res_local.start()

    def own_block(kind):
        if kind == 0:
            target = up_all.at[pl.ds(pl.multiple_of(me * depth, depth), depth)]
            return pltpu.make_async_copy(up_ref, target, local_sem.at[2])
        return pltpu.make_async_copy(down_ref, down_all.at[me], local_sem.at[3])

    @pl.when(home)
    def _():
        own_block(0).start()
        own_block(1).start()


    blocks = tokens // WINDOW
    heads_local = q_width // HEAD
    group = heads_local // (k_hbm.shape[1] // HEAD)

    slopes = [
        jnp.exp2(
            jnp.full((1, 2 * WINDOW), -8.0 / HEADS, jnp.float32)
            * (rank * heads_local + (h + 1)).astype(jnp.float32)
        )
        for h in range(heads_local)
    ]

    def windows(first_block, count):
        @pl.loop(0, count)
        def _(i):
            start = pl.multiple_of((first_block + i) * WINDOW, WINDOW)
            rows, span = pl.ds(start, WINDOW), pl.ds(start, 2 * WINDOW)
            q_index = lax.broadcasted_iota(jnp.int32, (WINDOW, 2 * WINDOW), 0)
            k_index = lax.broadcasted_iota(jnp.int32, (WINDOW, 2 * WINDOW), 1)
            dist = q_index + WINDOW - k_index
            key_pos = me * tokens + start - WINDOW + k_index
            valid = (dist >= 0) & (dist < WINDOW) & (key_pos >= 0)
            far = dist.astype(jnp.float32)
            for h in range(heads_local):
                columns = slice(h * HEAD, (h + 1) * HEAD)
                shared = slice(h // group * HEAD, (h // group + 1) * HEAD)
                logits = lax.dot_general(
                    q_ref[rows, columns], key_ext[span, shared], (((1,), (1,)), ((), ())),
                    preferred_element_type=jnp.float32,
                ) * HEAD ** (-0.5)
                logits = jnp.where(valid, logits - slopes[h] * far, neg_big)
                sink = sinks_ref[h]
                top = jnp.maximum(jnp.max(logits, axis=-1, keepdims=True), sink)
                probs = jnp.exp(logits - top)
                denom = jnp.sum(probs, axis=-1, keepdims=True) + jnp.exp(sink - top)
                weight = (probs / denom).astype(jnp.bfloat16)
                attended[rows, columns] = jnp.dot(
                    weight, val_ext[span, shared], preferred_element_type=jnp.float32
                ).astype(jnp.bfloat16)

    def rows_of(side, core):
        start = side * side_rows + core * own_rows
        return pl.ds(pl.multiple_of(start, own_rows), own_rows)

    def swap(i, side):
        return remote(
            attended.at[rows_of(side, oc)], att_in.at[i], att_send.at[i], att_recv.at[i],
            at(x, y, z, oc),
        )

    tile = 2 * LANES

    def project(i, side, target):
        @pl.loop(0, width // tile)
        def _(j):
            columns = pl.ds(pl.multiple_of(j * tile, tile), tile)
            target[:, columns] = (
                jnp.dot(
                    attended[rows_of(side, c)], proj_ref[:, columns],
                    preferred_element_type=jnp.float32,
                )
                + jnp.dot(att_in[i], proj_in[:, columns], preferred_element_type=jnp.float32)
            ).astype(target.dtype)

    part_rows = own_rows // ROW_PARTS

    def mix_copy(p):
        rows = pl.ds(p * part_rows, part_rows)
        return remote(
            mix_out.at[rows], mix_in.at[rows], mix_send.at[p], mix_recv.at[p], at(ox, y, z, c)
        )

    for copy in loads:
        copy.wait()
    windows(ox * (blocks // 2) + 1, blocks // 2 - 1)
    @pl.when(me != 0)
    def _():
        for copy in tails:
            copy.wait_recv()

    @pl.when(me == 0)
    def _():
        key_ext[:WINDOW] = jnp.zeros_like(key_ext[:WINDOW])
        val_ext[:WINDOW] = jnp.zeros_like(val_ext[:WINDOW])

    windows(ox * (blocks // 2), 1)
    swap(0, ox).start()
    proj_local.wait()
    proj_copy.wait_recv()
    swap(0, ox).wait_recv()
    project(0, ox, mix_out)
    for p in range(ROW_PARTS):
        mix_copy(p).start()
    windows(x * (blocks // 2), blocks // 2)
    swap(1, x).start()
    serve_z(0, 1)
    swap(1, x).wait_recv()
    project(1, x, mix_own)
    res_local.wait()

    def rank_rows(r, p):
        start = r * own_rows + p * part_rows
        return pl.ds(pl.multiple_of(start, part_rows), part_rows)

    def row_copy(t, p):
        source_ref, rows = normed_own.at[pl.ds(p * part_rows, part_rows)], rank_rows(rank, p)
        there = [at(x, y, z, oc), at(ox, y, z, zl), at(x, y, oz, zl)][t]
        return remote(
            source_ref, normed.at[rows], row_send.at[t, p], row_recv.at[rank, p], there
        )

    def row_in(side, core, p):
        r = side * CORES + core
        ref = normed.at[rank_rows(r, p)]
        return remote(ref, ref, fwd_send.at[core, p], row_recv.at[r, p], at(ox, y, z, c))

    for p in range(ROW_PARTS):
        mix_copy(p).wait_recv()

        @pl.loop(0, part_rows // step_rows)
        def _(i):
            start = pl.multiple_of(p * part_rows + i * step_rows, step_rows)
            rows = pl.ds(start, step_rows)
            mix = mix_own[rows] + mix_in[rows].astype(jnp.float32)
            stream = deep_alpha * res_ref[rows].astype(jnp.float32) + mix
            made = norm_rows(stream, gains_ref[0:1], biases_ref[0:1]).astype(jnp.bfloat16)
            normed_own[rows] = made

            @pl.when(home)
            def _():
                mine = pl.ds(pl.multiple_of(rank * own_rows + start, step_rows), step_rows)
                normed[mine] = made

        row_copy(2, p).start()
        row_copy(1, p).start()

        @pl.when(away)
        def _():
            row_copy(0, p).start()

    serve_z(0, 2)

    @pl.when(u == 0)
    def _():
        launch_local(1)

    @pl.when((u == 0) & away)
    def _():
        launch_main(1)

    serve_y(0, 0)
    serve_y(0, 1)

    serve_z(0, 3)

    @pl.when(((u == 1) & away) | ((u == 0) & home))
    def _():
        launch_main(1)

    @pl.when(u == 1)
    def _():
        launch_local(1)

    @pl.when(away)
    def _():
        for p in range(ROW_PARTS):
            for core in range(CORES):
                row_in(x, core, p).wait_recv()
                row_in(x, core, p).start()

    launch_extra(1)
    serve_y(0, 2)
    serve_y(0, 3)
    for k in range(LAYERS):
        for other in range(2):
            need(0, other, k)

    for p in range(ROW_PARTS):
        for core in range(CORES):
            row_in(ox, core, p).wait_recv()

        @pl.when(home)
        def _():
            row_in(x, oc, p).wait_recv()

    tiles = hidden // tile

    def upward(first, last):
        @pl.loop(first, last)
        def _(i):
            columns = pl.ds(pl.multiple_of(i * tile, tile), tile)
            made = jnp.dot(normed[...], up_all[:, columns], preferred_element_type=jnp.float32)
            act[:, columns] = jnp.square(jnp.maximum(made, 0.0)).astype(jnp.bfloat16)

    parts = 4
    for part in range(parts):
        upward(part * tiles // parts, (part + 1) * tiles // parts)
        if part == 0:
            @pl.when((u == 1) & home)
            def _():
                launch_main(1)

            serve_z(1, 1)

    @pl.when(u == 1)
    def _():
        for p in range(PIECES[1]):
            passed(1, p).start()

    steps = 2 * LAYERS

    def out_copy(i, t):
        r = [x * CORES + oc, ox * CORES, ox * CORES + 1][t]
        rows = pl.ds(pl.multiple_of(r * own_rows, own_rows), own_rows)
        there = [at(x, y, z, oc), at(ox, y, z, 0), at(ox, y, z, 1)][t]
        slot = 0 if t == 0 else 1
        return remote(
            terms.at[i, rows], terms_in.at[slot, i], out_send.at[i, t], out_recv.at[slot, i], there
        )

    def cross_copy(i):
        rows = pl.ds(pl.multiple_of(ox * side_rows, side_rows), side_rows)
        return remote(
            terms.at[i, rows], cross_in.at[i], cross_send.at[i], cross_recv.at[i], at(ox, y, z, c)
        )

    def join_copy(i, core):
        return remote(
            joined.at[i, pl.ds(core * own_rows, own_rows)], terms_in.at[2, i],
            join_send.at[i, core], out_recv.at[2, i], at(x, y, oz, core),
        )

    held_rows = pl.ds(pl.multiple_of(rank * own_rows, own_rows), own_rows)

    def downward(i):
        s = column(i // 2, i % 2)
        @pl.loop(0, 2)
        def _(r):
            rows = pl.ds(pl.multiple_of(r * (tokens // 2), tokens // 2), tokens // 2)
            terms[i, rows] = jnp.dot(
                act[rows], down_all[s], preferred_element_type=jnp.float32
            ).astype(jnp.bfloat16)

        @pl.when(home)
        def _():
            for t in range(3):
                out_copy(i, t).start()
            terms_in[0, i] = terms[i, held_rows]

        @pl.when(away)
        def _():
            cross_copy(i).start()

    def join(i):
        @pl.when(away)
        def _():
            cross_copy(i).wait_recv()
            rows = pl.ds(pl.multiple_of(x * side_rows, side_rows), side_rows)
            joined[i] = (
                terms[i, rows].astype(jnp.float32) + cross_in[i].astype(jnp.float32)
            ).astype(jnp.bfloat16)
            for core in range(CORES):
                join_copy(i, core).start()

    def collect(k):
        for other in range(2):
            i = 2 * k + other
            i2 = 2 * (1 - k if k < 2 else k) + other

            @pl.when(away)
            def _():
                out_copy(i, 0).wait_recv()

            out_copy(i, 1).wait_recv()
            join_copy(i2, 0).wait_recv()
            columns = pl.ds(pl.multiple_of(column(k, other) * depth, depth), depth)
            block = terms_in[0, i].astype(jnp.float32)
            block += terms_in[1, i].astype(jnp.float32)
            block += terms_in[2, i2].astype(jnp.float32)
            total[:, columns] = deep_alpha * normed_own[:, columns].astype(jnp.float32) + block

    before = {
        1: [(serve_y, 0)],
        2: [(serve_z, 2)],
        3: [(serve_y, 1)],
        4: [(serve_z, 3)],
        5: [(serve_y, 2)],
        7: [(serve_y, 3)],
    }
    for i in range(steps):
        k, other = i // 2, i % 2
        for serve, at_k in before.get(i, []):
            serve(1, at_k)
        need(1, other, k)
        downward(i)
        if i == 6:
            for j in range(i):
                join(j)
        if i > 6:
            join(i - 1)
    join(steps - 1)
    for k in range(LAYERS):
        collect(k)

    @pl.loop(0, own_rows // step_rows)
    def _(i):
        rows = pl.ds(pl.multiple_of(i * step_rows, step_rows), step_rows)
        out_ref[rows] = norm_rows(total[rows], gains_ref[1:2], biases_ref[1:2]).astype(jnp.bfloat16)

    @pl.when(me != n - 1)
    def _():
        for copy in tails:
            copy.wait_send()

    proj_copy.wait_send()
    swap(0, ox).wait_send()
    swap(1, x).wait_send()
    for p in range(ROW_PARTS):
        mix_copy(p).wait_send()
        row_copy(1, p).wait_send()
        row_copy(2, p).wait_send()
    for kind in range(2):
        for p in range(PIECES[kind]):
            for h in range(2):
                main(kind, h, p).wait_send()
            for k in range(LAYERS):
                if k > 0:
                    y_out(kind, k, p).wait_send()
                    across(kind, 0, k, p, c).wait_send()
                across(kind, 1, k, p, c).wait_send()

    @pl.when(extra_here)
    def _():
        for kind in range(2):
            for p in range(PIECES[kind]):
                for h in range(2):
                    extra(kind, h, p).wait_send()

    @pl.when(u == 1)
    def _():
        for kind in range(2):
            for p in range(PIECES[kind]):
                passed(kind, p).wait_send()

    @pl.when(home)
    def _():
        for kind in range(2):
            whole(kind).wait_send()
            for p in range(PIECES[kind]):
                for h in range(2):
                    first(kind, h, p).wait_send()
        for i in range(steps):
            for t in range(3):
                out_copy(i, t).wait_send()

    @pl.when(away)
    def _():
        for p in range(ROW_PARTS):
            row_copy(0, p).wait_send()
            for core in range(CORES):
                row_in(x, core, p).wait_send()
        for i in range(steps):
            cross_copy(i).wait_send()
            for core in range(CORES):
                join_copy(i, core).wait_send()


def fused_block(
    queries, keys, values, sinks, out_weight, up_weight, down_weight, residual, gains, biases
):
    n, m = lax.axis_size("sp"), lax.axis_size("tp")
    depth, hidden = up_weight.shape
    tokens = queries.shape[0]
    own_rows, width = residual.shape
    side_rows, steps = tokens // SIDES, 2 * LAYERS
    vmem, smem = pl.BlockSpec(memory_space=pltpu.VMEM), pl.BlockSpec(memory_space=pltpu.SMEM)
    bf16, dma = jnp.bfloat16, pltpu.SemaphoreType.DMA
    return pl.pallas_call(
        functools.partial(block_kernel, n, m),
        out_shape=jax.ShapeDtypeStruct(residual.shape, bf16),
        in_specs=[smem] + [vmem] * 2 + [pl.BlockSpec(memory_space=pl.ANY)] * 7,
        out_specs=pl.BlockSpec(memory_space=pltpu.VMEM),
        scratch_shapes=[
            pltpu.VMEM(queries.shape, bf16),
            pltpu.VMEM((tokens + WINDOW, keys.shape[1]), bf16),
            pltpu.VMEM((tokens + WINDOW, keys.shape[1]), bf16),
            pltpu.VMEM(out_weight.shape, bf16),
            pltpu.VMEM(residual.shape, bf16),
            pltpu.VMEM(queries.shape, bf16),
            pltpu.VMEM((SIDES, own_rows, queries.shape[1]), bf16),
            pltpu.VMEM(out_weight.shape, bf16),
            pltpu.VMEM((own_rows, width), bf16),
            pltpu.VMEM((own_rows, width), jnp.float32),
            pltpu.VMEM((own_rows, width), bf16),
            pltpu.VMEM((width, hidden), bf16),
            pltpu.VMEM((n, hidden, depth), bf16),
            pltpu.VMEM((own_rows, width), bf16),
            pltpu.VMEM((tokens, width), bf16),
            pltpu.VMEM((tokens, hidden), bf16),
            pltpu.VMEM((steps, tokens, depth), bf16),
            pltpu.VMEM((steps, side_rows, depth), bf16),
            pltpu.VMEM((steps, side_rows, depth), bf16),
            pltpu.VMEM((3, steps, own_rows, depth), bf16),
            pltpu.VMEM((own_rows, width), jnp.float32),
            dma((2,)),
            dma((2,)),
            dma((1,)),
            dma((1,)),
            dma((SIDES,)),
            dma((SIDES,)),
            dma((ROW_PARTS,)),
            dma((ROW_PARTS,)),
            dma((2, 2, max(PIECES))),
            dma((2, 2, max(PIECES))),
            dma((2, max(PIECES))),
            dma((2, LAYERS, max(PIECES))),
            dma((2, 2, max(PIECES))),
            dma((2, LAYERS, max(PIECES))),
            dma((2, LAYERS, max(PIECES))),
            dma((2,)),
            dma((2,)),
            dma((2, 2, LAYERS, max(PIECES))),
            dma((2, 2, LAYERS, max(PIECES))),
            dma((3, ROW_PARTS)),
            dma((m, ROW_PARTS)),
            dma((CORES, ROW_PARTS)),
            dma((steps, 3)),
            dma((steps,)),
            dma((steps,)),
            dma((steps, CORES)),
            dma((3, steps)),
            dma((7,)),
        ],
        compiler_params=pltpu.CompilerParams(
            collective_id=0, has_side_effects=True, vmem_limit_bytes=60 * 1024 * 1024
        ),
    )(
        sinks, gains, biases, queries, keys, values, out_weight, up_weight, down_weight, residual,
    )


def on_device(
    queries, keys, values, residual, sinks, out_weight, up_weight, down_weight, gains, biases
):
    tokens = queries.shape[0]
    rank_tp = lax.axis_index("tp")
    if fits(tokens, up_weight):
        return fused_block(
            queries, keys, values, sinks, out_weight, up_weight, down_weight, residual, gains, biases
        )
    tails = jnp.stack([keys[tokens - WINDOW :], values[tokens - WINDOW :]])
    before = from_behind(tails, "sp", 1)
    offset = lax.axis_index("sp") * tokens
    attended = attend(queries, keys, values, before, sinks, offset, rank_tp)
    part = jnp.dot(attended, out_weight, preferred_element_type=jnp.float32).astype(jnp.bfloat16)
    up_full, down_full = (
        lax.all_gather(up_weight, "sp", axis=0, tiled=True),
        lax.all_gather(down_weight, "sp", axis=1, tiled=True),
    )
    mix = lax.psum_scatter(
        part,
        "tp",
        scatter_dimension=0,
        tiled=True,
    ).astype(jnp.float32)
    normed = layer_norm(deep_alpha * residual.astype(jnp.float32) + mix, gains[0], biases[0])
    whole = lax.all_gather(normed, "tp", axis=0, tiled=True)
    upward = jnp.dot(whole, up_full, preferred_element_type=jnp.float32)
    act = jnp.square(jax.nn.relu(upward)).astype(jnp.bfloat16)
    terms = jnp.dot(act, down_full, preferred_element_type=jnp.float32)
    ffn = lax.psum_scatter(
        terms.astype(jnp.bfloat16), "tp", scatter_dimension=0, tiled=True
    ).astype(jnp.float32)
    return layer_norm(deep_alpha * normed.astype(jnp.float32) + ffn, gains[1], biases[1])


def solution(mesh):
    return jax.shard_map(
        on_device,
        mesh=mesh,
        in_specs=(
            P("sp", "tp"),
            P("sp", "tp"),
            P("sp", "tp"),
            P(("sp", "tp"), None),
            P("tp"),
            P("tp", None),
            P("sp", "tp"),
            P("tp", "sp"),
            P(),
            P(),
        ),
        out_specs=P(("sp", "tp"), None),
        check_vma=False,
    )
```
